256 devices in a mesh: tp: 16 (over y, x), dp: 16 (over z, core).
Axes of the slice: x: 4, y: 4, z: 8, core: 2. Of those that a mesh axis runs over, the one named last changes fastest.
Arguments:
- tokens: bfloat16 [256, 4096], P(None, 'dp'), may hold values from -15 to 15, as said below
- norm_gain: float32 [2, 4096], P(None, 'dp'), may hold values from 0.1 to 1.9
- w_query: bfloat16 [2, 4096, 2048], P(None, 'dp', 'tp'), may hold values from -0.09375 to 0.09375
- w_forget: bfloat16 [2, 4096, 2048], P(None, 'dp', 'tp'), may hold values from -0.09375 to 0.09375
- w_value: bfloat16 [2, 4096, 2048], P(None, 'dp', 'tp'), may hold values from -0.09375 to 0.09375
- w_gate: bfloat16 [2, 4096, 2048], P(None, 'dp', 'tp'), may hold values from -0.09375 to 0.09375
- floor_rate: float32 [2, 2048], P(None, 'tp'), may hold values from 0 to 0.9
- head_gain: float32 [2, 128], replicated, may hold values from 0.1 to 1.9
- w_output: bfloat16 [2, 2048, 4096], P(None, 'tp', 'dp'), may hold values from -0.3 to 0.3
- state: float32 [2, 256, 16, 128, 128], P(None, 'dp', 'tp'), may hold values from -4 to 4
Outputs:
- mixed: bfloat16 [256, 4096], P(None, 'dp')
- new_state: float32 [2, 256, 16, 128, 128], P(None, 'dp', 'tp')
The draws below stay inside these ranges and needn't reach their ends.
Inputs may be any that keep to these rules, and one draw needn't show every extreme that they name: `tokens`: activations whose feature blocks have different scales.
All inputs are finite; a program needn't handle non-finite values.
Results may differ from the reference program's by a relative error of at most 0.035.
Values may be sent and summed in bfloat16 or wider, within the bound.
No kernel may reach another device: no remote copies, remote signals or barrier semaphores. Data moves between devices by JAX's collectives and lax.ppermute only.
A program may use at most 64 MiB of HBM per device.

```python
import jax
import jax.numpy as jnp
from jax import lax

D = 4096
H = 16
DK = 128
DV = 128
BATCH = 256
N_DP = 16


def draw_tokens(key, part):
    first, second, third = jax.random.split(key, 3)
    group_scales = jnp.exp(jax.random.uniform(second, (32,), jnp.float32, jnp.log(0.25), jnp.log(2.5)))
    column_scales = jnp.repeat(group_scales, D // 32)
    base = jnp.clip(jax.random.normal(first, (BATCH, D), jnp.float32), -5.9, 5.9)
    return (base * column_scales[None, :]).astype(jnp.bfloat16)


def draw_w_output(key, part):
    rows = H * DV
    keys = jax.random.split(jax.random.fold_in(key, 71), 5)
    even_signs = 2.0 * jax.random.randint(keys[0], (2, rows, 1), 0, 2).astype(jnp.float32) - 1.0
    odd_signs = 2.0 * jax.random.randint(keys[1], (2, rows, 1), 0, 2).astype(jnp.float32) - 1.0
    column_signs = 2.0 * jax.random.randint(keys[2], (2, 1, D), 0, 2).astype(jnp.float32) - 1.0
    block_parity = (jnp.arange(D) // (D // N_DP) % 2)[None, None, :]
    pattern = jnp.where(block_parity == 0, even_signs, odd_signs)
    sigma = 1.5 / jnp.sqrt(jnp.float32(rows))
    magnitude = jax.random.uniform(keys[3], (2, 1, D), jnp.float32, 0.02, 0.06)
    noise = jnp.clip(jax.random.normal(keys[4], (2, rows, D), jnp.float32), -5.0, 5.0) * sigma
    total = jnp.clip(pattern * column_signs * magnitude + noise, -0.298, 0.298)
    return total.astype(jnp.bfloat16)


def block_scale(own_key, extent, cuts, low, largest):
    gain = 1.0
    for dim, parts in cuts:
        heights = jax.random.uniform(jax.random.fold_in(jax.random.fold_in(own_key, 6), dim), (parts,), jnp.float32, low / len(cuts), largest / len(cuts))
        gain = gain * jnp.repeat(jnp.exp(heights), extent[dim] // parts).reshape((-1,) + (1,) * (len(extent) - 1 - dim))
    return gain


def normal_values(own_key, extent, spread, limit, cuts=(), held_as=jnp.bfloat16):
    level = block_scale(own_key, extent, cuts, -0.22, 0.18) if cuts else 1.0
    array = jax.random.normal(own_key, extent, jnp.float32) * spread * level
    return jnp.minimum(jnp.maximum(array, -limit), limit).astype(held_as)


def setup_inputs(seed: int = 0) -> dict:
    streams_of = jax.random.split(jax.random.key(seed), 11)
    return {
        "tokens": draw_tokens(jax.random.fold_in(streams_of[10], 71), 0),
        "norm_gain": jnp.clip(1.0 + 0.18 * jax.random.normal(streams_of[1], (2, D), jnp.float32), 0.1, 1.9),
        "w_query": normal_values(streams_of[2], (2, D, H * DK), D ** -0.5, 0.09375, ((1, 16), (2, 16))),
        "w_forget": normal_values(streams_of[3], (2, D, H * DK), D ** -0.5, 0.09375, ((1, 16), (2, 16))),
        "w_value": normal_values(streams_of[4], (2, D, H * DV), D ** -0.5, 0.09375, ((1, 16), (2, 16))),
        "w_gate": normal_values(streams_of[5], (2, D, H * DV), D ** -0.5, 0.09375, ((1, 16), (2, 16))),
        "floor_rate": jnp.clip(0.9 * jax.random.uniform(streams_of[6], (2, H * DK), jnp.float32) ** block_scale(streams_of[6], (2, H * DK), ((1, 16),), -0.2, 0.2), 0.0, 0.9),
        "head_gain": jnp.clip(1.0 + 0.18 * jax.random.normal(streams_of[7], (2, DV), jnp.float32), 0.1, 1.9),
        "w_output": draw_w_output(jax.random.fold_in(streams_of[10], 71), 0),
        "state": normal_values(streams_of[9], (2, BATCH, H, DK, DV), 0.5, 4.0, ((1, 16), (2, 16)), jnp.float32),
    }


EPS = 1e-06

def mixer_layer(tokens, norm_gain, w_query, w_forget, w_value, w_gate, floor_rate, head_gain, w_output, old_state):
    tok = tokens.astype(jnp.float32)
    row_scale = lax.rsqrt(lax.optimization_barrier(jnp.mean(tok * tok, axis=-1, keepdims=True)) + EPS)
    normed = (tok * norm_gain).astype(jnp.bfloat16)
    blocks = normed.reshape(BATCH, N_DP, D // N_DP).astype(jnp.float32)

    def project(weight):
        pieces = weight.reshape(N_DP, D // N_DP, weight.shape[1]).astype(jnp.float32)
        partial_terms = jnp.einsum('bnd,ndc->nbc', blocks, pieces)
        rounded = lax.optimization_barrier(partial_terms.astype(jnp.bfloat16))
        total = lax.optimization_barrier(jnp.sum(rounded.astype(jnp.float32), axis=0))
        stored = lax.optimization_barrier((row_scale * total).astype(jnp.bfloat16))
        return stored.astype(jnp.float32).reshape(BATCH, H, -1)
    query = jax.nn.silu(project(w_query)) * DK ** (-0.5)
    forget_pre = project(w_forget)
    value = project(w_value)
    gate_pre = project(w_gate)
    floor_heads = floor_rate.reshape(H, DK)
    forget = floor_heads + (1.0 - floor_heads) * jax.nn.sigmoid(forget_pre)
    key_in = (1.0 - floor_heads) * jax.nn.sigmoid(-forget_pre)
    updated = old_state * forget[..., None] + key_in[..., None] * value[:, :, None, :]
    read = jnp.einsum('bhk,bhkv->bhv', query, updated, precision=lax.Precision.HIGHEST)
    read = read * lax.rsqrt(lax.optimization_barrier(jnp.mean(read * read, axis=-1, keepdims=True)) + EPS) * head_gain
    gated = (read * jax.nn.silu(gate_pre)).reshape(BATCH, H * DV).astype(jnp.bfloat16)
    update = jnp.dot(gated, w_output, preferred_element_type=jnp.float32)
    return ((tok + update).astype(jnp.bfloat16), updated)

def reference(tokens, norm_gain, w_query, w_forget, w_value, w_gate, floor_rate, head_gain, w_output, state):
    current = tokens
    states = []
    for layer_index in range(2):
        current, updated = mixer_layer(current, norm_gain[layer_index], w_query[layer_index], w_forget[layer_index], w_value[layer_index], w_gate[layer_index], floor_rate[layer_index], head_gain[layer_index], w_output[layer_index], state[layer_index])
        states.append(updated)
    return (current, jnp.stack(states, axis=0))
```

```python
import jax
import jax.numpy as jnp
from jax import lax
from jax.sharding import Mesh
from jax.sharding import PartitionSpec as P

D = 4096
DK = 128
EPS = 1e-06
BF16 = jnp.bfloat16
F32 = jnp.float32


def split_in_three(x):
    high = lax.reduce_precision(x, 8, 7)
    rest = x - high
    middle = lax.reduce_precision(rest, 8, 7)
    return high, middle, rest - middle


def per_device(
    tokens, norm_gain, w_query, w_forget, w_value, w_gate, floor_rate, head_gain, w_output, state
):
    n_z, n_x = lax.axis_size("z"), lax.axis_size("x")
    n_y = lax.axis_size("y")
    core = lax.axis_index("c")
    my_x = lax.axis_index("x")
    batch, feats = tokens.shape
    own_rows = batch // (2 * n_z)
    rows = n_z * own_rows

    def swap(v):
        return lax.ppermute(v, "c", [(0, 1), (1, 0)])

    tok = tokens.reshape(n_z, 2, own_rows, feats)
    mine = lax.dynamic_index_in_dim(tok, core, 1, keepdims=False).reshape(rows, feats)
    theirs = lax.dynamic_index_in_dim(tok, 1 - core, 1, keepdims=False).reshape(rows, feats)
    current = (mine, swap(theirs))

    w_in = jnp.concatenate([w_query, w_forget, w_value, w_gate], axis=2)
    w_in = (w_in, swap(w_in))
    gains = (norm_gain, swap(norm_gain))

    pieces = [w_output]
    for k in range(1, n_x):
        pieces.append(lax.ppermute(w_output, "x", [(i, (i + k) % n_x) for i in range(n_x)]))
    relative = jnp.stack(pieces)
    order = (my_x - jnp.arange(n_x)) % n_x
    gathered = jnp.stack(
        [lax.dynamic_index_in_dim(relative, order[i], 0, keepdims=False) for i in range(n_x)]
    )
    w_out = (gathered, swap(gathered))

    states = []
    for layer in range(2):
        total = jnp.zeros((rows, w_in[0].shape[2]), F32)
        squares = jnp.zeros((rows,), F32)
        for half in range(2):
            x = current[half].astype(F32)
            normed = (x * gains[half][layer][None, :]).astype(BF16)
            total += jnp.dot(normed, w_in[half][layer], preferred_element_type=F32)
            squares += jnp.sum(x * x, axis=1)
        high, middle, low = split_in_three(squares)
        lane = lax.broadcasted_iota(jnp.int32, (rows, 128), 1)
        extra = jnp.where(
            lane == 0,
            high[:, None],
            jnp.where(lane == 1, middle[:, None], jnp.where(lane == 2, low[:, None], 0.0)),
        )
        payload = jnp.concatenate([total, extra], axis=1).astype(BF16).reshape(n_z, own_rows, -1)
        arrived = lax.all_to_all(payload, "z", split_axis=0, concat_axis=0, tiled=True)
        summed = arrived.astype(F32).sum(axis=0)
        square = summed[:, 512] + summed[:, 513] + summed[:, 514]
        row_scale = lax.rsqrt(square / D + EPS)
        stored = row_scale[:, None] * summed[:, :512]
        query = jax.nn.silu(stored[:, :128]) * DK ** (-0.5)
        forget_pre = stored[:, 128:256]
        value = stored[:, 256:384]
        gate_pre = stored[:, 384:512]
        floor = floor_rate[layer][None, :]
        forget = floor + (1.0 - floor) * jax.nn.sigmoid(forget_pre)
        key_in = (1.0 - floor) * jax.nn.sigmoid(-forget_pre)
        old = state[layer][:, 0]
        updated = old * forget[:, :, None] + key_in[:, :, None] * value[:, None, :]
        states.append(updated[:, None])
        read = jnp.sum(query[:, :, None] * updated, axis=1)
        read = read * lax.rsqrt(jnp.mean(read * read, axis=-1, keepdims=True) + EPS)
        gated = (read * head_gain[layer][None, :] * jax.nn.silu(gate_pre)).astype(BF16)

        copies = jnp.broadcast_to(gated, (n_x * n_z, *gated.shape))
        heads = lax.all_to_all(copies, ("x", "z"), split_axis=0, concat_axis=0, tiled=True)
        heads = heads.reshape(n_x, rows, -1)
        partial = [
            jnp.einsum("xsk,xkf->sf", heads, w_out[half][:, layer], preferred_element_type=F32)
            for half in range(2)
        ]
        partial = jnp.concatenate(partial, axis=1).astype(BF16)
        copies = jnp.broadcast_to(partial, (n_y, *partial.shape))
        parts = lax.all_to_all(copies, "y", split_axis=0, concat_axis=0, tiled=True)
        update = parts.astype(F32).sum(axis=0)
        current = tuple(
            (current[half].astype(F32) + update[:, half * feats : (half + 1) * feats]).astype(BF16)
            for half in range(2)
        )
    other = swap(current[1]).reshape(n_z, own_rows, feats)
    own = current[0].reshape(n_z, own_rows, feats)
    first = jnp.where(core == 0, own, other)
    second = jnp.where(core == 0, other, own)
    mixed = jnp.stack([first, second], axis=1).reshape(batch, feats)
    return mixed, jnp.stack(states, axis=0)


def solution(mesh):
    n_tp, n_dp = mesh.devices.shape
    fine = Mesh(mesh.devices.reshape(4, n_tp // 4, n_dp // 2, 2), ("y", "x", "z", "c"))
    dp, tp = ("z", "c"), ("y", "x")
    in_specs = (
        P(None, dp),
        P(None, dp),
        P(None, dp, tp),
        P(None, dp, tp),
        P(None, dp, tp),
        P(None, dp, tp),
        P(None, tp),
        P(),
        P(None, tp, dp),
        P(None, dp, tp, None, None),
    )
    out_specs = (P(None, dp), P(None, dp, tp, None, None))
    return jax.shard_map(
        per_device, mesh=fine, in_specs=in_specs, out_specs=out_specs, check_vma=False
    )
```

```python
import functools

import jax
import jax.numpy as jnp
from jax import lax
from jax.experimental import pallas as pl
from jax.experimental.pallas import tpu as pltpu
from jax.sharding import Mesh
from jax.sharding import PartitionSpec as P

D = 4096
EPS = 1e-06
BF16 = jnp.bfloat16
F32 = jnp.float32
LANES = 128


def call(kernel, outs, *args, flops=0, name=None):
    vmem = pl.BlockSpec(memory_space=pltpu.VMEM)
    size = sum(a.size * a.dtype.itemsize for a in args)
    return pl.pallas_call(
        kernel,
        out_shape=outs,
        in_specs=[vmem] * len(args),
        out_specs=[vmem] * len(outs),
        cost_estimate=pl.CostEstimate(flops=flops, bytes_accessed=size, transcendentals=0),
        compiler_params=pltpu.CompilerParams(vmem_limit_bytes=12 * 2**20),
        name=name,
    )(*args)


def rounded(x):
    return x.astype(BF16).astype(F32)


def pack(halves, gains, weights, layer, payload_ref):
    n_z, own_rows, _ = payload_ref.shape
    rows = n_z * own_rows
    totals = [None] * 4
    squares = None
    for half in range(2):
        x = halves[half].astype(F32)
        normed = (x * gains[half][layer : layer + 1, :]).astype(BF16)
        for p in range(4):
            product = jnp.dot(normed, weights[half][p][layer], preferred_element_type=F32)
            totals[p] = product if totals[p] is None else totals[p] + product
        square = jnp.sum(x * x, axis=1, keepdims=True)
        squares = square if squares is None else squares + square
    for p in range(4):
        payload_ref[:, :, p * LANES : (p + 1) * LANES] = (
            totals[p].astype(BF16).reshape(n_z, own_rows, LANES)
        )
    high = rounded(squares)
    middle = rounded(squares - high)
    low = squares - high - middle
    lane = lax.broadcasted_iota(jnp.int32, (rows, LANES), 1)
    extra = jnp.where(
        lane == 0, high, jnp.where(lane == 1, middle, jnp.where(lane == 2, low, 0.0))
    )
    payload_ref[:, :, 4 * LANES :] = extra.astype(BF16).reshape(n_z, own_rows, LANES)


def first_kernel(tok_b, gain_b, *refs):
    w_b, (tok_a, gain_a), w_a = refs[0:4], refs[4:6], refs[6:10]
    payload_ref, x_ref, tok_mine, gain_mine, w_mine, sems = refs[10:]
    core = lax.axis_index("c")
    n_z, _, own_rows, feats = tok_b.shape
    copies = [
        pltpu.make_async_copy(tok_a.at[:, core], tok_mine, sems.at[0]),
        pltpu.make_async_copy(gain_a, gain_mine, sems.at[1]),
        *[pltpu.make_async_copy(w_a[p].at[0:1], w_mine.at[p], sems.at[2 + p]) for p in range(4)],
    ]
    for copy in copies:
        copy.start()
    x_ref[1] = tok_b[:, core].reshape(n_z * own_rows, feats)
    for copy in copies:
        copy.wait()
    x_ref[0] = tok_mine[...].reshape(n_z * own_rows, feats)
    weights = ([w_mine.at[p] for p in range(4)], w_b)
    pack([x_ref[0], x_ref[1]], (gain_mine, gain_b), weights, 0, payload_ref)


def first(payload_shape, x_shape, own, other):
    vmem = pl.BlockSpec(memory_space=pltpu.VMEM)
    hbm = pl.BlockSpec(memory_space=pltpu.HBM)
    n_z, _, own_rows, feats = own[0].shape
    return pl.pallas_call(
        first_kernel,
        out_shape=[payload_shape, x_shape],
        in_specs=[vmem] * len(other) + [hbm] * len(own),
        out_specs=[vmem, vmem],
        scratch_shapes=[
            pltpu.VMEM((n_z, own_rows, feats), BF16),
            pltpu.VMEM(own[1].shape, F32),
            pltpu.VMEM((4, 1, *own[2].shape[1:]), BF16),
            pltpu.SemaphoreType.DMA((6,)),
        ],
        cost_estimate=pl.CostEstimate(flops=10**8, bytes_accessed=10**6, transcendentals=0),
        compiler_params=pltpu.CompilerParams(vmem_limit_bytes=12 * 2**20),
        name="first",
    )(*other, *own)


def add_up(parts, x_ref, feats):
    terms = [p[...].astype(F32) for p in parts]
    update = (terms[0] + terms[1]) + (terms[2] + terms[3])
    return [
        (x_ref[half].astype(F32) + update[:, half * feats : (half + 1) * feats]).astype(BF16)
        for half in range(2)
    ]


def middle_kernel(layer, *refs):
    parts, (x_in, gain_a, gain_b), weights = refs[0:4], refs[4:7], (refs[7:11], refs[11:15])
    payload_ref, x_ref = refs[15:]
    halves = add_up(parts, x_in, x_in.shape[2])
    x_ref[0] = halves[0]
    x_ref[1] = halves[1]
    pack(halves, (gain_a, gain_b), weights, layer, payload_ref)


def last_kernel(*refs):
    parts, (x_in, keep_ref, send_ref) = refs[0:4], refs[4:]
    halves = add_up(parts, x_in, x_in.shape[2])
    keep_ref[...] = halves[0]
    send_ref[...] = halves[1]


def join_kernel(keep, received, out_ref):
    core = lax.axis_index("c")
    n_z, _, own_rows, feats = out_ref.shape
    out_ref[:, core] = keep[...].reshape(n_z, own_rows, feats)
    out_ref[:, 1 - core] = received[...].reshape(n_z, own_rows, feats)


def sigmoid(x):
    return 1.0 / (1.0 + jnp.exp(-x))


def mix_kernel(layer, arrived, floor_rate, head_gain, state, gated_ref, terms_ref):
    summed = arrived[0].astype(F32)
    for n in range(1, arrived.shape[0]):
        summed = summed + arrived[n].astype(F32)
    own_rows = summed.shape[0]
    extra = summed[:, 4 * LANES :]
    square = extra[:, 0:1] + extra[:, 1:2] + extra[:, 2:3]
    row_scale = lax.rsqrt(square / D + EPS)
    query_pre, forget_pre, value, gate_pre = [
        row_scale * summed[:, p * LANES : (p + 1) * LANES] for p in range(4)
    ]
    floor = floor_rate[layer : layer + 1, :]
    query = query_pre * sigmoid(query_pre) * LANES ** (-0.5)
    forget = floor + (1.0 - floor) * sigmoid(forget_pre)
    key_in = (1.0 - floor) * sigmoid(-forget_pre)
    terms_ref[0] = forget
    terms_ref[1] = key_in
    terms_ref[2] = value
    columns = (query * forget).T
    fresh = jnp.sum(query * key_in, axis=1, keepdims=True) * value
    kept = [
        jnp.sum(state[layer, i, 0] * columns[:, i : i + 1], axis=0, keepdims=True)
        for i in range(own_rows)
    ]
    read = jnp.concatenate(kept, axis=0) + fresh
    read = read * lax.rsqrt(jnp.mean(read * read, axis=1, keepdims=True) + EPS)
    gate = gate_pre * sigmoid(gate_pre)
    gated = (read * head_gain[layer : layer + 1, :] * gate).astype(BF16)
    for n in range(gated_ref.shape[0]):
        gated_ref[n] = gated


def update_kernel(terms_a, terms_b, state, out_ref):
    def write(terms):
        forget = terms[0].T
        key_in = terms[1].T
        for i in range(state.shape[1]):
            value = terms[2, i : i + 1, :]
            out_ref[0, i, 0] = state[0, i, 0] * forget[:, i : i + 1] + key_in[:, i : i + 1] * value

    @pl.when(pl.program_id(0) == 0)
    def _():
        write(terms_a)

    @pl.when(pl.program_id(0) == 1)
    def _():
        write(terms_b)


def new_states(terms_a, terms_b, state):
    layers, seqs, heads, dk, dv = state.shape
    step = 8
    terms_spec = pl.BlockSpec((3, step, dk), lambda l, i: (0, i, 0))
    state_spec = pl.BlockSpec((1, step, heads, dk, dv), lambda l, i: (l, i, 0, 0, 0))
    return pl.pallas_call(
        update_kernel,
        out_shape=jax.ShapeDtypeStruct(state.shape, F32),
        grid=(layers, seqs // step),
        in_specs=[terms_spec, terms_spec, state_spec],
        out_specs=state_spec,
        cost_estimate=pl.CostEstimate(flops=10**7, bytes_accessed=2 * state.size * 4, transcendentals=0),
        compiler_params=pltpu.CompilerParams(vmem_limit_bytes=12 * 2**20),
        name="new_states",
    )(terms_a, terms_b, state)


def output_kernel(layer, heads, w_a, w_b, out_ref):
    my_x = lax.axis_index("x")
    n_x = heads.shape[0]
    rows = heads.shape[1] * heads.shape[2]
    for half, w in enumerate((w_a, w_b)):
        total = None
        for i in range(n_x):
            block = w[lax.rem(my_x - i + n_x, n_x), layer]
            product = jnp.dot(
                heads[i].reshape(rows, LANES), block, preferred_element_type=F32
            )
            total = product if total is None else total + product
        total = total.astype(BF16)
        feats = total.shape[1]
        out_ref[:, half * feats : (half + 1) * feats] = total


def spread(copies, axes):
    return lax.all_to_all(copies, axes, split_axis=0, concat_axis=0, tiled=True)


def per_device(
    tokens, norm_gain, w_query, w_forget, w_value, w_gate, floor_rate, head_gain, w_output, state
):
    n_z, n_x, n_y = lax.axis_size("z"), lax.axis_size("x"), lax.axis_size("y")
    batch, feats = tokens.shape
    own_rows = batch // (2 * n_z)
    rows = n_z * own_rows

    def swap(v):
        return lax.ppermute(v, "c", [(0, 1), (1, 0)])

    weights = (w_query, w_forget, w_value, w_gate)
    tok = tokens.reshape(n_z, 2, own_rows, feats)
    others = (swap(tok), swap(norm_gain), *[swap(w) for w in weights])
    projections = (norm_gain, others[1], *weights, *others[2:])

    payload_shape = jax.ShapeDtypeStruct((n_z, own_rows, 5 * LANES), BF16)
    x_shape = jax.ShapeDtypeStruct((2, rows, feats), BF16)
    payload, x = first(payload_shape, x_shape, (tok, norm_gain, *weights), others)

    payload, w_late = lax.optimization_barrier((payload, w_output))
    pieces = [w_output]
    for k in range(1, n_x):
        pieces.append(lax.ppermute(w_late, "x", [(i, (i + k) % n_x) for i in range(n_x)]))
    gathered = jnp.stack(pieces)
    w_out = (gathered, swap(gathered))

    terms = []
    for layer in range(2):
        arrived = spread(payload, "z")
        gated, term = call(
            functools.partial(mix_kernel, layer),
            [
                jax.ShapeDtypeStruct((n_x * n_z, own_rows, LANES), BF16),
                jax.ShapeDtypeStruct((3, own_rows, LANES), F32),
            ],
            arrived, floor_rate, head_gain, state, flops=10**7, name=f"mix_{layer}",
        )
        terms.append(term)
        heads = spread(gated, ("x", "z")).reshape(n_x, n_z, own_rows, LANES)
        (own,) = call(
            functools.partial(output_kernel, layer),
            [jax.ShapeDtypeStruct((rows, 2 * feats), BF16)],
            heads, *w_out, flops=10**8, name=f"output_{layer}",
        )
        parts = [own]
        for k in range(1, n_y):
            parts.append(lax.ppermute(own, "y", [(i, i ^ k) for i in range(n_y)]))
        if layer == 0:
            payload, x = call(
                functools.partial(middle_kernel, 1), [payload_shape, x_shape],
                *parts, x, *projections, flops=10**8, name="middle",
            )
    half = jax.ShapeDtypeStruct((rows, feats), BF16)
    keep, send = call(last_kernel, [half, half], *parts, x, flops=10**6, name="last")
    (mixed,) = call(
        join_kernel, [jax.ShapeDtypeStruct((n_z, 2, own_rows, feats), BF16)],
        keep, swap(send), flops=10**6, name="join",
    )
    return mixed.reshape(batch, feats), new_states(*terms, state)


def solution(mesh):
    n_tp, n_dp = mesh.devices.shape
    fine = Mesh(mesh.devices.reshape(4, n_tp // 4, n_dp // 2, 2), ("y", "x", "z", "c"))
    dp, tp = ("z", "c"), ("y", "x")
    in_specs = (
        P(None, dp),
        P(None, dp),
        P(None, dp, tp),
        P(None, dp, tp),
        P(None, dp, tp),
        P(None, dp, tp),
        P(None, tp),
        P(),
        P(None, tp, dp),
        P(None, dp, tp, None, None),
    )
    out_specs = (P(None, dp), P(None, dp, tp, None, None))
    return jax.shard_map(
        per_device, mesh=fine, in_specs=in_specs, out_specs=out_specs, check_vma=False
    )
```

```python
import functools

import jax
import jax.numpy as jnp
from jax import lax
from jax.experimental import pallas as pl
from jax.experimental.pallas import tpu as pltpu
from jax.sharding import Mesh
from jax.sharding import PartitionSpec as P


D = 4096
EPS = 1e-06
BF16 = jnp.bfloat16
F32 = jnp.float32
LANES = 128


START_LIMIT = 56 * 2**20


def call(kernel, outs, *args, flops=0):
    vmem = pl.BlockSpec(memory_space=pltpu.VMEM)
    size = sum(a.size * a.dtype.itemsize for a in args)
    return pl.pallas_call(
        kernel,
        out_shape=outs,
        in_specs=[vmem] * len(args),
        out_specs=[vmem] * len(outs),
        cost_estimate=pl.CostEstimate(flops=flops, bytes_accessed=size, transcendentals=0),
        compiler_params=pltpu.CompilerParams(vmem_limit_bytes=12 * 2**20),
    )(*args)


def rounded(x):
    return x.astype(BF16).astype(F32)


def project(x, gain, weights):
    x = x.astype(F32)
    normed = (x * gain).astype(BF16)
    products = [jnp.dot(normed, w, preferred_element_type=F32) for w in weights]
    return products, jnp.sum(x * x, axis=1, keepdims=True)


def in_three(squares):
    high = rounded(squares)
    middle = rounded(squares - high)
    low = squares - high - middle
    lane = lax.broadcasted_iota(jnp.int32, (squares.shape[0], LANES), 1)
    return jnp.where(
        lane == 0, high, jnp.where(lane == 1, middle, jnp.where(lane == 2, low, 0.0))
    )


def store(totals, squares, payload_ref):
    n_z, own_rows, _ = payload_ref.shape
    for p, part in enumerate([*totals, in_three(squares)]):
        payload_ref[:, :, p * LANES : (p + 1) * LANES] = (
            part.astype(BF16).reshape(n_z, own_rows, LANES)
        )


def start_kernel(tok, gain, floor_rate, head_gain, *refs):
    w = refs[0:4]
    keep_ref, send_ref, bundle_ref, tok_here, gain_here, rates_here, w_here, sems = refs[4:]
    core = lax.axis_index("c")
    n_z, _, own_rows, feats = tok.shape
    rows = n_z * own_rows
    copies = [
        pltpu.make_async_copy(tok, tok_here, sems.at[0]),
        pltpu.make_async_copy(gain, gain_here, sems.at[1]),
        pltpu.make_async_copy(floor_rate, rates_here.at[0], sems.at[2]),
        pltpu.make_async_copy(head_gain, rates_here.at[1], sems.at[3]),
        *[pltpu.make_async_copy(w[p], w_here.at[p], sems.at[4 + p]) for p in range(4)],
    ]
    for copy in copies:
        copy.start()
    for copy in copies:
        copy.wait()
    weights = [w_here.at[p] for p in range(4)]
    gain_0 = gain_here[0:1, :]
    x = tok_here[:, 1 - core].reshape(rows, feats)
    bundle_ref[0:rows, 4 * LANES :] = x
    store(*project(x, gain_0, [v[0] for v in weights]), send_ref)
    x = tok_here[:, core].reshape(rows, feats)
    totals, squares = project(x, gain_0, [v[0] for v in weights])
    for p in range(4):
        keep_ref[0:rows, p * LANES : (p + 1) * LANES] = totals[p]
        bundle_ref[0:feats, p * LANES : (p + 1) * LANES] = weights[p][1]
    keep_ref[0:rows, 4 * LANES :] = in_three(squares)
    keep_ref[rows : rows + 2, 0:LANES] = rates_here[0]
    keep_ref[rows + 2 : rows + 4, 0:LANES] = rates_here[1]
    gain_1 = gain_here[1:2, :]
    high = rounded(gain_1)
    middle = rounded(gain_1 - high)
    for n, term in enumerate((high, middle, gain_1 - high - middle)):
        bundle_ref[rows + 16 * n : rows + 16 * n + 16, 4 * LANES :] = jnp.broadcast_to(
            term, (16, feats)
        ).astype(BF16)


def start(payload_shape, rows, *own):
    vmem = pl.BlockSpec(memory_space=pltpu.VMEM)
    hbm = pl.BlockSpec(memory_space=pltpu.HBM)
    feats = own[1].shape[1]
    return pl.pallas_call(
        start_kernel,
        out_shape=[
            jax.ShapeDtypeStruct((rows + 8, 5 * LANES), F32),
            payload_shape,
            jax.ShapeDtypeStruct((feats, 4 * LANES + feats), BF16),
        ],
        in_specs=[hbm] * len(own),
        out_specs=[vmem] * 3,
        scratch_shapes=[
            pltpu.VMEM(own[0].shape, BF16),
            pltpu.VMEM(own[1].shape, F32),
            pltpu.VMEM((2, *own[2].shape), F32),
            pltpu.VMEM((4, *own[4].shape), BF16),
            pltpu.SemaphoreType.DMA((8,)),
        ],
        cost_estimate=pl.CostEstimate(flops=10**8, bytes_accessed=10**6, transcendentals=0),
        compiler_params=pltpu.CompilerParams(vmem_limit_bytes=START_LIMIT),
        name="start",
    )(*own)


def pair_kernel(keep, received, payload_ref, rates_ref):
    n_z, own_rows, width = received.shape
    rates_ref[...] = keep[n_z * own_rows :, 0:LANES]
    total = keep[0 : n_z * own_rows, :] + received[...].reshape(n_z * own_rows, width).astype(F32)
    extra = total[:, 4 * LANES :]
    squares = extra[:, 0:1] + extra[:, 1:2] + extra[:, 2:3]
    store([total[:, p * LANES : (p + 1) * LANES] for p in range(4)], squares, payload_ref)


def add_up(parts, halves):
    terms = [p[...].astype(F32) for p in parts]
    update = (terms[0] + terms[1]) + (terms[2] + terms[3])
    feats = halves[0].shape[1]
    return [
        (half.astype(F32) + update[:, n * feats : (n + 1) * feats]).astype(BF16)
        for n, half in enumerate(halves)
    ]


def middle_kernel(p0, p1, p2, p3, tok, bundle_a, bundle_b, payload_ref, x_ref):
    core = lax.axis_index("c")
    n_z, _, own_rows, feats = tok.shape
    rows = n_z * own_rows
    mine = tok[:, core].reshape(rows, feats)
    halves = add_up((p0, p1, p2, p3), [mine, bundle_b[0:rows, 4 * LANES :]])
    results = []
    for half, bundle in zip(halves, (bundle_a, bundle_b)):
        gain = sum(
            bundle[rows + 16 * n : rows + 16 * n + 16, 4 * LANES :][0:1].astype(F32)
            for n in range(3)
        )
        weights = [bundle[:, p * LANES : (p + 1) * LANES] for p in range(4)]
        results.append(project(half, gain, weights))
    (totals, squares), (others, other_squares) = results
    store([t + o for t, o in zip(totals, others)], squares + other_squares, payload_ref)
    x_ref[0] = halves[0]
    x_ref[1] = halves[1]


def last_kernel(*refs):
    parts, (x_in, keep_ref, send_ref) = refs[0:4], refs[4:]
    halves = add_up(parts, [x_in[0], x_in[1]])
    keep_ref[...] = halves[0]
    send_ref[...] = halves[1]


def join_kernel(keep, received, out_ref):
    core = lax.axis_index("c")
    n_z, _, own_rows, feats = out_ref.shape
    out_ref[:, core] = keep[...].reshape(n_z, own_rows, feats)
    out_ref[:, 1 - core] = received[...].reshape(n_z, own_rows, feats)


def sigmoid(x):
    return 1.0 / (1.0 + jnp.exp(-x))


def mix_kernel(layer, arrived, rates, state, gated_ref, terms_ref):
    summed = arrived[0].astype(F32)
    for n in range(1, arrived.shape[0]):
        summed = summed + arrived[n].astype(F32)
    own_rows = summed.shape[0]
    extra = summed[:, 4 * LANES :]
    square = extra[:, 0:1] + extra[:, 1:2] + extra[:, 2:3]
    row_scale = lax.rsqrt(square / D + EPS)
    query_pre, forget_pre, value, gate_pre = [
        row_scale * summed[:, p * LANES : (p + 1) * LANES] for p in range(4)
    ]
    floor = rates[layer : layer + 1, :]
    query = query_pre * sigmoid(query_pre) * LANES ** (-0.5)
    forget = floor + (1.0 - floor) * sigmoid(forget_pre)
    key_in = (1.0 - floor) * sigmoid(-forget_pre)
    terms_ref[0] = forget
    terms_ref[1] = key_in
    terms_ref[2] = value
    columns = (query * forget).T
    fresh = jnp.sum(query * key_in, axis=1, keepdims=True) * value
    kept = [
        jnp.sum(state[layer, i, 0] * columns[:, i : i + 1], axis=0, keepdims=True)
        for i in range(own_rows)
    ]
    read = jnp.concatenate(kept, axis=0) + fresh
    read = read * lax.rsqrt(jnp.mean(read * read, axis=1, keepdims=True) + EPS)
    gate = gate_pre * sigmoid(gate_pre)
    gated = (read * rates[layer + 2 : layer + 3, :] * gate).astype(BF16)
    for n in range(gated_ref.shape[0]):
        gated_ref[n] = gated


def update_kernel(terms_a, terms_b, state, out_ref):
    def write(terms):
        forget = terms[0].T
        key_in = terms[1].T
        for i in range(state.shape[1]):
            value = terms[2, i : i + 1, :]
            out_ref[0, i, 0] = state[0, i, 0] * forget[:, i : i + 1] + key_in[:, i : i + 1] * value

    @pl.when(pl.program_id(0) == 0)
    def _():
        write(terms_a)

    @pl.when(pl.program_id(0) == 1)
    def _():
        write(terms_b)


def new_states(terms_a, terms_b, state):
    layers, seqs, heads, dk, dv = state.shape
    step = 8
    terms_spec = pl.BlockSpec((3, step, dk), lambda l, i: (0, i, 0))
    state_spec = pl.BlockSpec((1, step, heads, dk, dv), lambda l, i: (l, i, 0, 0, 0))
    return pl.pallas_call(
        update_kernel,
        out_shape=jax.ShapeDtypeStruct(state.shape, F32),
        grid=(layers, seqs // step),
        in_specs=[terms_spec, terms_spec, state_spec],
        out_specs=state_spec,
        cost_estimate=pl.CostEstimate(flops=10**7, bytes_accessed=2 * state.size * 4, transcendentals=0),
        compiler_params=pltpu.CompilerParams(vmem_limit_bytes=12 * 2**20),
        name="new_states",
    )(terms_a, terms_b, state)


def output_kernel(layer, heads, w_a, w_b, out_ref):
    my_x = lax.axis_index("x")
    n_x = heads.shape[0]
    rows = heads.shape[1] * heads.shape[2]
    for half, w in enumerate((w_a, w_b)):
        total = None
        for i in range(n_x):
            block = w[lax.rem(my_x - i + n_x, n_x), layer]
            product = jnp.dot(
                heads[i].reshape(rows, LANES), block, preferred_element_type=F32
            )
            total = product if total is None else total + product
        total = total.astype(BF16)
        feats = total.shape[1]
        out_ref[:, half * feats : (half + 1) * feats] = total


def spread(copies, axes):
    return lax.all_to_all(copies, axes, split_axis=0, concat_axis=0, tiled=True)


def per_device(
    tokens, norm_gain, w_query, w_forget, w_value, w_gate, floor_rate, head_gain, w_output, state
):
    n_z, n_x, n_y = lax.axis_size("z"), lax.axis_size("x"), lax.axis_size("y")
    batch, feats = tokens.shape
    own_rows = batch // (2 * n_z)
    rows = n_z * own_rows

    def swap(v):
        return lax.ppermute(v, "c", [(0, 1), (1, 0)])

    weights = (w_query, w_forget, w_value, w_gate)
    tok = tokens.reshape(n_z, 2, own_rows, feats)
    payload_shape = jax.ShapeDtypeStruct((n_z, own_rows, 5 * LANES), BF16)
    x_shape = jax.ShapeDtypeStruct((2, rows, feats), BF16)
    keep, send, bundle = start(
        payload_shape, rows, tok, norm_gain, floor_rate, head_gain, *weights
    )
    received = swap(send)
    payload, rates = call(
        pair_kernel, [payload_shape, jax.ShapeDtypeStruct((8, LANES), F32)],
        keep, received, flops=10**6,
    )
    bundle_b = swap(bundle)
    pieces = [w_output]
    for k in range(1, n_x):
        pieces.append(lax.ppermute(w_output, "x", [(i, (i + k) % n_x) for i in range(n_x)]))
    gathered = jnp.stack(pieces)
    w_out = (gathered, swap(gathered))

    terms = []
    for layer in range(2):
        arrived = spread(payload, "z")
        gated, term = call(
            functools.partial(mix_kernel, layer),
            [
                jax.ShapeDtypeStruct((n_x * n_z, own_rows, LANES), BF16),
                jax.ShapeDtypeStruct((3, own_rows, LANES), F32),
            ],
            arrived, rates, state, flops=10**7,
        )
        terms.append(term)
        heads = spread(gated, ("x", "z")).reshape(n_x, n_z, own_rows, LANES)
        (own,) = call(
            functools.partial(output_kernel, layer),
            [jax.ShapeDtypeStruct((rows, 2 * feats), BF16)],
            heads, *w_out, flops=10**8,
        )
        parts = [own]
        for k in range(1, n_y):
            parts.append(lax.ppermute(own, "y", [(i, i ^ k) for i in range(n_y)]))
        if layer == 0:
            payload, x = call(
                middle_kernel, [payload_shape, x_shape],
                *parts, tok, bundle, bundle_b, flops=10**8,
            )
    half = jax.ShapeDtypeStruct((rows, feats), BF16)
    keep, send = call(last_kernel, [half, half], *parts, x, flops=10**6)
    states = new_states(*terms, state)
    received = swap(send)
    (mixed,) = call(
        join_kernel, [jax.ShapeDtypeStruct((n_z, 2, own_rows, feats), BF16)],
        keep, received, flops=10**6,
    )
    return mixed.reshape(batch, feats), states


def solution(mesh):
    n_tp, n_dp = mesh.devices.shape
    fine = Mesh(mesh.devices.reshape(4, n_tp // 4, n_dp // 2, 2), ("y", "x", "z", "c"))
    dp, tp = ("z", "c"), ("y", "x")
    in_specs = (
        P(None, dp),
        P(None, dp),
        P(None, dp, tp),
        P(None, dp, tp),
        P(None, dp, tp),
        P(None, dp, tp),
        P(None, tp),
        P(),
        P(None, tp, dp),
        P(None, dp, tp, None, None),
    )
    out_specs = (P(None, dp), P(None, dp, tp, None, None))
    return jax.shard_map(
        per_device, mesh=fine, in_specs=in_specs, out_specs=out_specs, check_vma=False
    )
```

```python
import functools

import jax
import jax.numpy as jnp
from jax import lax
from jax.experimental import pallas as pl
from jax.experimental.pallas import tpu as pltpu
from jax.sharding import Mesh
from jax.sharding import PartitionSpec as P


D = 4096
EPS = 1e-06
BF16 = jnp.bfloat16
F32 = jnp.float32
LANES = 128


START_LIMIT = 56 * 2**20


def call(kernel, outs, *args, flops=0):
    vmem = pl.BlockSpec(memory_space=pltpu.VMEM)
    size = sum(a.size * a.dtype.itemsize for a in args)
    return pl.pallas_call(
        kernel,
        out_shape=outs,
        in_specs=[vmem] * len(args),
        out_specs=[vmem] * len(outs),
        cost_estimate=pl.CostEstimate(flops=flops, bytes_accessed=size, transcendentals=0),
        compiler_params=pltpu.CompilerParams(vmem_limit_bytes=12 * 2**20),
    )(*args)


def rounded(x):
    return x.astype(BF16).astype(F32)


def project(x, gain, weights):
    x = x.astype(F32)
    normed = (x * gain).astype(BF16)
    products = [jnp.dot(normed, w, preferred_element_type=F32) for w in weights]
    return products, jnp.sum(x * x, axis=1, keepdims=True)


def in_three(squares):
    high = rounded(squares)
    middle = rounded(squares - high)
    low = squares - high - middle
    lane = lax.broadcasted_iota(jnp.int32, (squares.shape[0], LANES), 1)
    return jnp.where(
        lane == 0, high, jnp.where(lane == 1, middle, jnp.where(lane == 2, low, 0.0))
    )


def store(totals, squares, payload_ref):
    n_z, own_rows, _ = payload_ref.shape
    for p, part in enumerate([*totals, in_three(squares)]):
        payload_ref[:, :, p * LANES : (p + 1) * LANES] = (
            part.astype(BF16).reshape(n_z, own_rows, LANES)
        )


def start_kernel(tok, gain, *refs):
    w = refs[0:4]
    payload_ref, bundle_ref, tok_here, gain_here, w_here, sems = refs[4:]
    core = lax.axis_index("c")
    n_z, _, own_rows, feats = tok.shape
    rows = n_z * own_rows
    copies = [
        pltpu.make_async_copy(tok, tok_here, sems.at[0]),
        pltpu.make_async_copy(gain, gain_here, sems.at[1]),
        *[pltpu.make_async_copy(w[p], w_here.at[p], sems.at[2 + p]) for p in range(4)],
    ]
    for copy in copies:
        copy.start()
    for copy in copies:
        copy.wait()
    weights = [w_here.at[p] for p in range(4)]
    x = tok_here[...].reshape(2 * rows, feats)
    store(*project(x, gain_here[0:1, :], [v[0] for v in weights]), payload_ref)
    for p in range(4):
        bundle_ref[:, p * LANES : (p + 1) * LANES] = weights[p][1]
    bundle_ref[0:rows, 4 * LANES :] = tok_here[:, 1 - core].reshape(rows, feats)
    gain_1 = gain_here[1:2, :]
    high = rounded(gain_1)
    middle = rounded(gain_1 - high)
    for n, term in enumerate((high, middle, gain_1 - high - middle)):
        bundle_ref[rows + 16 * n : rows + 16 * n + 16, 4 * LANES :] = jnp.broadcast_to(
            term, (16, feats)
        ).astype(BF16)


def start(n_dp, own_rows, *own):
    vmem = pl.BlockSpec(memory_space=pltpu.VMEM)
    hbm = pl.BlockSpec(memory_space=pltpu.HBM)
    feats = own[1].shape[1]
    return pl.pallas_call(
        start_kernel,
        out_shape=[
            jax.ShapeDtypeStruct((n_dp, own_rows, 5 * LANES), BF16),
            jax.ShapeDtypeStruct((feats, 4 * LANES + feats), BF16),
        ],
        in_specs=[hbm] * len(own),
        out_specs=[vmem] * 2,
        scratch_shapes=[
            pltpu.VMEM(own[0].shape, BF16),
            pltpu.VMEM(own[1].shape, F32),
            pltpu.VMEM((4, *own[2].shape), BF16),
            pltpu.SemaphoreType.DMA((6,)),
        ],
        cost_estimate=pl.CostEstimate(flops=10**8, bytes_accessed=10**6, transcendentals=0),
        compiler_params=pltpu.CompilerParams(vmem_limit_bytes=START_LIMIT),
        name="start",
    )(*own)


def rates_kernel(floor_rate, head_gain, out_ref):
    out_ref[0:2] = floor_rate[...]
    out_ref[2:4] = head_gain[...]


def add_up(parts, halves):
    terms = [p[...].astype(F32) for p in parts]
    update = (terms[0] + terms[1]) + (terms[2] + terms[3])
    feats = halves[0].shape[1]
    return [
        (half.astype(F32) + update[:, n * feats : (n + 1) * feats]).astype(BF16)
        for n, half in enumerate(halves)
    ]


def middle_kernel(p0, p1, p2, p3, tok, gain, *refs):
    w, (bundle, payload_ref, x_ref) = refs[0:4], refs[4:]
    core = lax.axis_index("c")
    n_z, _, own_rows, feats = tok.shape
    rows = n_z * own_rows
    mine = tok[:, core].reshape(rows, feats)
    halves = add_up((p0, p1, p2, p3), [mine, bundle[0:rows, 4 * LANES :]])
    other_gain = sum(
        bundle[rows + 16 * n : rows + 16 * n + 16, 4 * LANES :][0:1].astype(F32) for n in range(3)
    )
    totals, squares = project(halves[0], gain[1:2, :], [v[1] for v in w])
    other_w = [bundle[:, p * LANES : (p + 1) * LANES] for p in range(4)]
    others, other_squares = project(halves[1], other_gain, other_w)
    store([t + o for t, o in zip(totals, others)], squares + other_squares, payload_ref)
    x_ref[0] = halves[0]
    x_ref[1] = halves[1]


def last_kernel(*refs):
    parts, (x_in, keep_ref, send_ref) = refs[0:4], refs[4:]
    halves = add_up(parts, [x_in[0], x_in[1]])
    keep_ref[...] = halves[0]
    send_ref[...] = halves[1]


def join_kernel(keep, received, out_ref):
    core = lax.axis_index("c")
    n_z, _, own_rows, feats = out_ref.shape
    out_ref[:, core] = keep[...].reshape(n_z, own_rows, feats)
    out_ref[:, 1 - core] = received[...].reshape(n_z, own_rows, feats)


def sigmoid(x):
    return 1.0 / (1.0 + jnp.exp(-x))


def mix_kernel(layer, arrived, rates, state, gated_ref, terms_ref):
    summed = arrived[0].astype(F32)
    for n in range(1, arrived.shape[0]):
        summed = summed + arrived[n].astype(F32)
    own_rows = summed.shape[0]
    extra = summed[:, 4 * LANES :]
    square = extra[:, 0:1] + extra[:, 1:2] + extra[:, 2:3]
    row_scale = lax.rsqrt(square / D + EPS)
    query_pre, forget_pre, value, gate_pre = [
        row_scale * summed[:, p * LANES : (p + 1) * LANES] for p in range(4)
    ]
    floor = rates[layer : layer + 1, :]
    query = query_pre * sigmoid(query_pre) * LANES ** (-0.5)
    forget = floor + (1.0 - floor) * sigmoid(forget_pre)
    key_in = (1.0 - floor) * sigmoid(-forget_pre)
    terms_ref[0] = forget
    terms_ref[1] = key_in
    terms_ref[2] = value
    columns = (query * forget).T
    fresh = jnp.sum(query * key_in, axis=1, keepdims=True) * value
    kept = [
        jnp.sum(state[layer, i, 0] * columns[:, i : i + 1], axis=0, keepdims=True)
        for i in range(own_rows)
    ]
    read = jnp.concatenate(kept, axis=0) + fresh
    read = read * lax.rsqrt(jnp.mean(read * read, axis=1, keepdims=True) + EPS)
    gate = gate_pre * sigmoid(gate_pre)
    gated = (read * rates[layer + 2 : layer + 3, :] * gate).astype(BF16)
    for n in range(gated_ref.shape[0]):
        gated_ref[n] = gated


def update_kernel(terms_a, terms_b, state, out_ref):
    def write(terms):
        forget = terms[0].T
        key_in = terms[1].T
        for i in range(state.shape[1]):
            value = terms[2, i : i + 1, :]
            out_ref[0, i, 0] = state[0, i, 0] * forget[:, i : i + 1] + key_in[:, i : i + 1] * value

    @pl.when(pl.program_id(0) == 0)
    def _():
        write(terms_a)

    @pl.when(pl.program_id(0) == 1)
    def _():
        write(terms_b)


def new_states(terms_a, terms_b, state):
    layers, seqs, heads, dk, dv = state.shape
    step = 8
    terms_spec = pl.BlockSpec((3, step, dk), lambda l, i: (0, i, 0))
    state_spec = pl.BlockSpec((1, step, heads, dk, dv), lambda l, i: (l, i, 0, 0, 0))
    return pl.pallas_call(
        update_kernel,
        out_shape=jax.ShapeDtypeStruct(state.shape, F32),
        grid=(layers, seqs // step),
        in_specs=[terms_spec, terms_spec, state_spec],
        out_specs=state_spec,
        cost_estimate=pl.CostEstimate(flops=10**7, bytes_accessed=2 * state.size * 4, transcendentals=0),
        compiler_params=pltpu.CompilerParams(vmem_limit_bytes=12 * 2**20),
        name="new_states",
    )(terms_a, terms_b, state)


def output_kernel(layer, heads, w_a, w_b, out_ref):
    my_x = lax.axis_index("x")
    n_x = heads.shape[0]
    rows = heads.shape[1] * heads.shape[2]
    for half, w in enumerate((w_a, w_b)):
        total = None
        for i in range(n_x):
            block = w[lax.rem(my_x - i + n_x, n_x), layer]
            product = jnp.dot(
                heads[i].reshape(rows, LANES), block, preferred_element_type=F32
            )
            total = product if total is None else total + product
        total = total.astype(BF16)
        feats = total.shape[1]
        out_ref[:, half * feats : (half + 1) * feats] = total


def spread(copies, axes):
    return lax.all_to_all(copies, axes, split_axis=0, concat_axis=0, tiled=True)


def per_device(
    tokens, norm_gain, w_query, w_forget, w_value, w_gate, floor_rate, head_gain, w_output, state
):
    n_z, n_x, n_y = lax.axis_size("z"), lax.axis_size("x"), lax.axis_size("y")
    batch, feats = tokens.shape
    own_rows = batch // (2 * n_z)
    rows = n_z * own_rows

    def swap(v):
        return lax.ppermute(v, "c", [(0, 1), (1, 0)])

    weights = (w_query, w_forget, w_value, w_gate)
    tok = tokens.reshape(n_z, 2, own_rows, feats)
    payload_shape = jax.ShapeDtypeStruct((n_z, own_rows, 5 * LANES), BF16)
    x_shape = jax.ShapeDtypeStruct((2, rows, feats), BF16)
    payload, bundle = start(2 * n_z, own_rows, tok, norm_gain, *weights)
    (rates,) = call(
        rates_kernel, [jax.ShapeDtypeStruct((8, LANES), F32)],
        floor_rate, head_gain, flops=10**4,
    )
    bundle_b = swap(bundle)
    pieces = [w_output]
    for k in range(1, n_x):
        pieces.append(lax.ppermute(w_output, "x", [(i, (i + k) % n_x) for i in range(n_x)]))
    gathered = jnp.stack(pieces)
    w_out = (gathered, swap(gathered))

    terms = []
    for layer in range(2):
        arrived = spread(payload, ("z", "c") if layer == 0 else "z")
        gated, term = call(
            functools.partial(mix_kernel, layer),
            [
                jax.ShapeDtypeStruct((n_x * n_z, own_rows, LANES), BF16),
                jax.ShapeDtypeStruct((3, own_rows, LANES), F32),
            ],
            arrived, rates, state, flops=10**7,
        )
        terms.append(term)
        heads = spread(gated, ("x", "z")).reshape(n_x, n_z, own_rows, LANES)
        (own,) = call(
            functools.partial(output_kernel, layer),
            [jax.ShapeDtypeStruct((rows, 2 * feats), BF16)],
            heads, *w_out, flops=10**8,
        )
        parts = [own]
        for k in range(1, n_y):
            parts.append(lax.ppermute(own, "y", [(i, i ^ k) for i in range(n_y)]))
        if layer == 0:
            payload, x = call(
                middle_kernel, [payload_shape, x_shape],
                *parts, tok, norm_gain, *weights, bundle_b, flops=10**8,
            )
    half = jax.ShapeDtypeStruct((rows, feats), BF16)
    keep, send = call(last_kernel, [half, half], *parts, x, flops=10**6)
    states = new_states(*terms, state)
    received = swap(send)
    (mixed,) = call(
        join_kernel, [jax.ShapeDtypeStruct((n_z, 2, own_rows, feats), BF16)],
        keep, received, flops=10**6,
    )
    return mixed.reshape(batch, feats), states


def solution(mesh):
    n_tp, n_dp = mesh.devices.shape
    fine = Mesh(mesh.devices.reshape(4, n_tp // 4, n_dp // 2, 2), ("y", "x", "z", "c"))
    dp, tp = ("z", "c"), ("y", "x")
    in_specs = (
        P(None, dp),
        P(None, dp),
        P(None, dp, tp),
        P(None, dp, tp),
        P(None, dp, tp),
        P(None, dp, tp),
        P(None, tp),
        P(),
        P(None, tp, dp),
        P(None, dp, tp, None, None),
    )
    out_specs = (P(None, dp), P(None, dp, tp, None, None))
    return jax.shard_map(
        per_device, mesh=fine, in_specs=in_specs, out_specs=out_specs, check_vma=False
    )
```

```python
import functools

import jax
import jax.numpy as jnp
from jax import lax
from jax.experimental import pallas as pl
from jax.experimental.pallas import tpu as pltpu
from jax.sharding import Mesh
from jax.sharding import PartitionSpec as P


D = 4096
EPS = 1e-06
BF16 = jnp.bfloat16
F32 = jnp.float32
LANES = 128


START_LIMIT = 56 * 2**20


def call(kernel, outs, *args, flops=0):
    vmem = pl.BlockSpec(memory_space=pltpu.VMEM)
    size = sum(a.size * a.dtype.itemsize for a in args)
    return pl.pallas_call(
        kernel,
        out_shape=outs,
        in_specs=[vmem] * len(args),
        out_specs=[vmem] * len(outs),
        cost_estimate=pl.CostEstimate(flops=flops, bytes_accessed=size, transcendentals=0),
        compiler_params=pltpu.CompilerParams(vmem_limit_bytes=12 * 2**20),
    )(*args)


def rounded(x):
    return x.astype(BF16).astype(F32)


def project(x, gain, weights):
    x = x.astype(F32)
    normed = (x * gain).astype(BF16)
    products = [jnp.dot(normed, w, preferred_element_type=F32) for w in weights]
    return products, jnp.sum(x * x, axis=1, keepdims=True)


def in_three(squares):
    high = rounded(squares)
    middle = rounded(squares - high)
    low = squares - high - middle
    lane = lax.broadcasted_iota(jnp.int32, (squares.shape[0], LANES), 1)
    return jnp.where(
        lane == 0, high, jnp.where(lane == 1, middle, jnp.where(lane == 2, low, 0.0))
    )


def store(totals, squares, payload_ref):
    n_z, own_rows, _ = payload_ref.shape
    for p, part in enumerate([*totals, in_three(squares)]):
        payload_ref[:, :, p * LANES : (p + 1) * LANES] = (
            part.astype(BF16).reshape(n_z, own_rows, LANES)
        )


def start_kernel(tok, gain, w_output, *refs):
    w = refs[0:4]
    payload_ref, bundle_ref, out_0, tok_here, gain_here, w_here, o_here, sems = refs[4:]
    core = lax.axis_index("c")
    n_z, _, own_rows, feats = tok.shape
    rows = n_z * own_rows
    copies = [
        pltpu.make_async_copy(tok, tok_here, sems.at[0]),
        pltpu.make_async_copy(gain, gain_here, sems.at[1]),
        *[pltpu.make_async_copy(w[p], w_here.at[p], sems.at[2 + p]) for p in range(4)],
        pltpu.make_async_copy(w_output.at[0:1], o_here, sems.at[6]),
    ]
    for copy in copies:
        copy.start()
    for copy in copies:
        copy.wait()
    weights = [w_here.at[p] for p in range(4)]
    x = tok_here[...].reshape(2 * rows, feats)
    store(*project(x, gain_here[0:1, :], [v[0] for v in weights]), payload_ref)
    out_0[...] = o_here[0]
    for p in range(4):
        bundle_ref[:, p * LANES : (p + 1) * LANES] = weights[p][1]
    bundle_ref[0:rows, 4 * LANES :] = tok_here[:, 1 - core].reshape(rows, feats)
    gain_1 = gain_here[1:2, :]
    high = rounded(gain_1)
    middle = rounded(gain_1 - high)
    for n, term in enumerate((high, middle, gain_1 - high - middle)):
        bundle_ref[rows + 16 * n : rows + 16 * n + 16, 4 * LANES :] = jnp.broadcast_to(
            term, (16, feats)
        ).astype(BF16)


def start(n_dp, own_rows, *own):
    vmem = pl.BlockSpec(memory_space=pltpu.VMEM)
    hbm = pl.BlockSpec(memory_space=pltpu.HBM)
    feats = own[1].shape[1]
    return pl.pallas_call(
        start_kernel,
        out_shape=[
            jax.ShapeDtypeStruct((n_dp, own_rows, 5 * LANES), BF16),
            jax.ShapeDtypeStruct((feats, 4 * LANES + feats), BF16),
            jax.ShapeDtypeStruct(own[2].shape[1:], BF16),
        ],
        in_specs=[hbm] * len(own),
        out_specs=[vmem] * 3,
        scratch_shapes=[
            pltpu.VMEM(own[0].shape, BF16),
            pltpu.VMEM(own[1].shape, F32),
            pltpu.VMEM((4, *own[3].shape), BF16),
            pltpu.VMEM((1, *own[2].shape[1:]), BF16),
            pltpu.SemaphoreType.DMA((7,)),
        ],
        cost_estimate=pl.CostEstimate(flops=10**8, bytes_accessed=10**6, transcendentals=0),
        compiler_params=pltpu.CompilerParams(vmem_limit_bytes=START_LIMIT),
        name="start",
    )(*own)


def rates_kernel(floor_rate, head_gain, state, out_ref):
    out_ref[0:2] = floor_rate[...]
    out_ref[2:4] = head_gain[...]


def add_up(parts, halves):
    terms = [p[...].astype(F32) for p in parts]
    update = (terms[0] + terms[1]) + (terms[2] + terms[3])
    feats = halves[0].shape[1]
    return [
        (half.astype(F32) + update[:, n * feats : (n + 1) * feats]).astype(BF16)
        for n, half in enumerate(halves)
    ]


def middle_kernel(p0, p1, p2, p3, tok, gain, *refs):
    w, (bundle, payload_ref, keep_ref, send_ref) = refs[0:4], refs[4:]
    core = lax.axis_index("c")
    n_z, _, own_rows, feats = tok.shape
    rows = n_z * own_rows
    mine = tok[:, core].reshape(rows, feats)
    halves = add_up((p0, p1, p2, p3), [mine, bundle[0:rows, 4 * LANES :]])
    other_gain = sum(
        bundle[rows + 16 * n : rows + 16 * n + 16, 4 * LANES :][0:1].astype(F32) for n in range(3)
    )
    totals, squares = project(halves[0], gain[1:2, :], [v[1] for v in w])
    other_w = [bundle[:, p * LANES : (p + 1) * LANES] for p in range(4)]
    others, other_squares = project(halves[1], other_gain, other_w)
    store([t + o for t, o in zip(totals, others)], squares + other_squares, payload_ref)
    keep_ref[...] = halves[0]
    send_ref[...] = halves[1]


def last_kernel(p0, p1, p2, p3, x_keep, x_other, out_ref):
    core = lax.axis_index("c")
    for parity, x in ((core, x_keep), (1 - core, x_other)):
        a, b, c, d = [p[:, parity].astype(F32) for p in (p0, p1, p2, p3)]
        n_z, own_rows, feats = a.shape
        before = x[...].reshape(n_z, own_rows, feats).astype(F32)
        out_ref[:, parity] = (before + ((a + b) + (c + d))).astype(BF16)


def sigmoid(x):
    return 1.0 / (1.0 + jnp.exp(-x))


def mix_kernel(layer, arrived, rates, state, gated_ref, terms_ref):
    summed = arrived[0].astype(F32)
    for n in range(1, arrived.shape[0]):
        summed = summed + arrived[n].astype(F32)
    own_rows = summed.shape[0]
    extra = summed[:, 4 * LANES :]
    square = extra[:, 0:1] + extra[:, 1:2] + extra[:, 2:3]
    row_scale = lax.rsqrt(square / D + EPS)
    query_pre, forget_pre, value, gate_pre = [
        row_scale * summed[:, p * LANES : (p + 1) * LANES] for p in range(4)
    ]
    floor = rates[layer : layer + 1, :]
    query = query_pre * sigmoid(query_pre) * LANES ** (-0.5)
    forget = floor + (1.0 - floor) * sigmoid(forget_pre)
    key_in = (1.0 - floor) * sigmoid(-forget_pre)
    terms_ref[0] = forget
    terms_ref[1] = key_in
    terms_ref[2] = value
    columns = (query * forget).T
    fresh = jnp.sum(query * key_in, axis=1, keepdims=True) * value
    kept = [
        jnp.sum(state[layer, i, 0] * columns[:, i : i + 1], axis=0, keepdims=True)
        for i in range(own_rows)
    ]
    read = jnp.concatenate(kept, axis=0) + fresh
    read = read * lax.rsqrt(jnp.mean(read * read, axis=1, keepdims=True) + EPS)
    gate = gate_pre * sigmoid(gate_pre)
    gated = (read * rates[layer + 2 : layer + 3, :] * gate).astype(BF16)
    for n in range(gated_ref.shape[0]):
        gated_ref[n] = gated


def update_kernel(terms_a, terms_b, state, out_ref):
    def write(terms):
        forget = terms[0].T
        key_in = terms[1].T
        for i in range(state.shape[1]):
            value = terms[2, i : i + 1, :]
            out_ref[0, i, 0] = state[0, i, 0] * forget[:, i : i + 1] + key_in[:, i : i + 1] * value

    @pl.when(pl.program_id(0) == 0)
    def _():
        write(terms_a)

    @pl.when(pl.program_id(0) == 1)
    def _():
        write(terms_b)


def new_states(terms_a, terms_b, state):
    layers, seqs, heads, dk, dv = state.shape
    step = 8
    terms_spec = pl.BlockSpec((3, step, dk), lambda l, i: (0, i, 0))
    state_spec = pl.BlockSpec((1, step, heads, dk, dv), lambda l, i: (l, i, 0, 0, 0))
    return pl.pallas_call(
        update_kernel,
        out_shape=jax.ShapeDtypeStruct(state.shape, F32),
        grid=(layers, seqs // step),
        in_specs=[terms_spec, terms_spec, state_spec],
        out_specs=state_spec,
        cost_estimate=pl.CostEstimate(flops=10**7, bytes_accessed=2 * state.size * 4, transcendentals=0),
        compiler_params=pltpu.CompilerParams(vmem_limit_bytes=12 * 2**20),
        name="new_states",
    )(terms_a, terms_b, state)


def output_kernel(heads, w_a, w_b, out_ref):
    my_x = lax.axis_index("x")
    n_x = heads.shape[0]
    rows = heads.shape[1] * heads.shape[2]
    for half, w in enumerate((w_a, w_b)):
        total = None
        for i in range(n_x):
            block = w[lax.rem(my_x - i + n_x, n_x)]
            product = jnp.dot(
                heads[i].reshape(rows, LANES), block, preferred_element_type=F32
            )
            total = product if total is None else total + product
        total = total.astype(BF16)
        feats = total.shape[1]
        out_ref[:, half * feats : (half + 1) * feats] = total


def last_output_kernel(heads, other_heads, *refs):
    pieces, out_ref = refs[:-1], refs[-1]
    core = lax.axis_index("c")
    my_x = lax.axis_index("x")
    n_x, n_z, own_rows, _ = heads.shape
    for parity, h in ((core, heads), (1 - core, other_heads)):
        total = None
        for k in range(n_x):
            rows = h[lax.rem(my_x - k + n_x, n_x)].reshape(n_z * own_rows, LANES)
            product = jnp.dot(rows, pieces[k][1], preferred_element_type=F32)
            total = product if total is None else total + product
        out_ref[:, parity] = total.astype(BF16).reshape(n_z, own_rows, total.shape[1])


def spread(copies, axes):
    return lax.all_to_all(copies, axes, split_axis=0, concat_axis=0, tiled=True)


def per_device(
    tokens, norm_gain, w_query, w_forget, w_value, w_gate, floor_rate, head_gain, w_output, state
):
    n_z, n_x, n_y = lax.axis_size("z"), lax.axis_size("x"), lax.axis_size("y")
    batch, feats = tokens.shape
    own_rows = batch // (2 * n_z)
    rows = n_z * own_rows

    def swap(v):
        return lax.ppermute(v, "c", [(0, 1), (1, 0)])

    weights = (w_query, w_forget, w_value, w_gate)
    tok = tokens.reshape(n_z, 2, own_rows, feats)
    payload_shape = jax.ShapeDtypeStruct((n_z, own_rows, 5 * LANES), BF16)
    payload, bundle, w_out_0 = start(2 * n_z, own_rows, tok, norm_gain, w_output, *weights)
    (rates,) = call(
        rates_kernel, [jax.ShapeDtypeStruct((8, LANES), F32)],
        floor_rate, head_gain, state, flops=10**4,
    )
    bundle_b = swap(bundle)

    def gather(w):
        return [
            lax.ppermute(w, "x", [(i, (i + k) % n_x) for i in range(n_x)]) for k in range(1, n_x)
        ]

    pieces = [w_out_0, *gather(w_out_0)]
    gathered = jnp.stack(pieces)
    w_out = (gathered, swap(gathered))
    late = [w_output, *gather(w_output)]

    terms = []
    for layer in range(2):
        arrived = spread(payload, ("z", "c") if layer == 0 else "z")
        gated, term = call(
            functools.partial(mix_kernel, layer),
            [
                jax.ShapeDtypeStruct((n_x * n_z, own_rows, LANES), BF16),
                jax.ShapeDtypeStruct((3, own_rows, LANES), F32),
            ],
            arrived, rates, state, flops=10**7,
        )
        terms.append(term)
        heads = spread(gated, ("x", "z")).reshape(n_x, n_z, own_rows, LANES)
        if layer == 0:
            shape = jax.ShapeDtypeStruct((rows, 2 * feats), BF16)
            operands = (output_kernel, [shape], heads, *w_out)
        else:
            other_heads = swap(heads)
            shape = jax.ShapeDtypeStruct((n_z, 2, own_rows, feats), BF16)
            operands = (last_output_kernel, [shape], heads, other_heads, *late)
        (own,) = call(*operands, flops=10**8)
        parts = [own]
        for k in range(1, n_y):
            parts.append(lax.ppermute(own, "y", [(i, i ^ k) for i in range(n_y)]))
        if layer == 0:
            half = jax.ShapeDtypeStruct((rows, feats), BF16)
            payload, x_keep, x_send = call(
                middle_kernel, [payload_shape, half, half],
                *parts, tok, norm_gain, *weights, bundle_b, flops=10**8,
            )
    x_other = swap(x_send)
    (mixed,) = call(
        last_kernel, [jax.ShapeDtypeStruct((n_z, 2, own_rows, feats), BF16)],
        *parts, x_keep, x_other, flops=10**6,
    )
    states = new_states(*terms, state)
    return mixed.reshape(batch, feats), states


def solution(mesh):
    n_tp, n_dp = mesh.devices.shape
    fine = Mesh(mesh.devices.reshape(4, n_tp // 4, n_dp // 2, 2), ("y", "x", "z", "c"))
    dp, tp = ("z", "c"), ("y", "x")
    in_specs = (
        P(None, dp),
        P(None, dp),
        P(None, dp, tp),
        P(None, dp, tp),
        P(None, dp, tp),
        P(None, dp, tp),
        P(None, tp),
        P(),
        P(None, tp, dp),
        P(None, dp, tp, None, None),
    )
    out_specs = (P(None, dp), P(None, dp, tp, None, None))
    return jax.shard_map(
        per_device, mesh=fine, in_specs=in_specs, out_specs=out_specs, check_vma=False
    )
```

```python
import functools

import jax
import jax.numpy as jnp
from jax import lax
from jax.experimental import pallas as pl
from jax.experimental.pallas import tpu as pltpu
from jax.sharding import Mesh
from jax.sharding import PartitionSpec as P


D = 4096
EPS = 1e-06
BF16 = jnp.bfloat16
F32 = jnp.float32
LANES = 128


START_LIMIT = 56 * 2**20


def call(kernel, outs, *args, flops=0):
    vmem = pl.BlockSpec(memory_space=pltpu.VMEM)
    size = sum(a.size * a.dtype.itemsize for a in args)
    return pl.pallas_call(
        kernel,
        out_shape=outs,
        in_specs=[vmem] * len(args),
        out_specs=[vmem] * len(outs),
        cost_estimate=pl.CostEstimate(flops=flops, bytes_accessed=size, transcendentals=0),
        compiler_params=pltpu.CompilerParams(vmem_limit_bytes=12 * 2**20),
    )(*args)


def rounded(x):
    return x.astype(BF16).astype(F32)


def project(x, gain, weights):
    x = x.astype(F32)
    normed = (x * gain).astype(BF16)
    products = [jnp.dot(normed, w, preferred_element_type=F32) for w in weights]
    return products, jnp.sum(x * x, axis=1, keepdims=True)


def in_three(squares):
    high = rounded(squares)
    middle = rounded(squares - high)
    low = squares - high - middle
    lane = lax.broadcasted_iota(jnp.int32, (squares.shape[0], LANES), 1)
    return jnp.where(
        lane == 0, high, jnp.where(lane == 1, middle, jnp.where(lane == 2, low, 0.0))
    )


def store(totals, squares, payload_ref):
    n_z, own_rows, _ = payload_ref.shape
    for p, part in enumerate([*totals, in_three(squares)]):
        payload_ref[:, :, p * LANES : (p + 1) * LANES] = (
            part.astype(BF16).reshape(n_z, own_rows, LANES)
        )


def start_kernel(tok, gain, floor_rate, head_gain, *refs):
    w = refs[0:4]
    keep_ref, send_ref, bundle_ref, tok_here, gain_here, rates_here, w_here, sems = refs[4:]
    core = lax.axis_index("c")
    n_z, _, own_rows, feats = tok.shape
    rows = n_z * own_rows
    copies = [
        pltpu.make_async_copy(tok, tok_here, sems.at[0]),
        pltpu.make_async_copy(gain, gain_here, sems.at[1]),
        pltpu.make_async_copy(floor_rate, rates_here.at[0], sems.at[2]),
        pltpu.make_async_copy(head_gain, rates_here.at[1], sems.at[3]),
        *[pltpu.make_async_copy(w[p], w_here.at[p], sems.at[4 + p]) for p in range(4)],
    ]
    for copy in copies:
        copy.start()
    for copy in copies:
        copy.wait()
    weights = [w_here.at[p] for p in range(4)]
    gain_0 = gain_here[0:1, :]
    x = tok_here[:, 1 - core].reshape(rows, feats)
    bundle_ref[0:rows, 4 * LANES :] = x
    store(*project(x, gain_0, [v[0] for v in weights]), send_ref)
    x = tok_here[:, core].reshape(rows, feats)
    totals, squares = project(x, gain_0, [v[0] for v in weights])
    for p in range(4):
        keep_ref[0:rows, p * LANES : (p + 1) * LANES] = totals[p]
        bundle_ref[0:feats, p * LANES : (p + 1) * LANES] = weights[p][1]
    keep_ref[0:rows, 4 * LANES :] = in_three(squares)
    keep_ref[rows : rows + 2, 0:LANES] = rates_here[0]
    keep_ref[rows + 2 : rows + 4, 0:LANES] = rates_here[1]
    gain_1 = gain_here[1:2, :]
    high = rounded(gain_1)
    middle = rounded(gain_1 - high)
    for n, term in enumerate((high, middle, gain_1 - high - middle)):
        bundle_ref[rows + 16 * n : rows + 16 * n + 16, 4 * LANES :] = jnp.broadcast_to(
            term, (16, feats)
        ).astype(BF16)


def start(payload_shape, rows, *own):
    vmem = pl.BlockSpec(memory_space=pltpu.VMEM)
    hbm = pl.BlockSpec(memory_space=pltpu.HBM)
    feats = own[1].shape[1]
    return pl.pallas_call(
        start_kernel,
        out_shape=[
            jax.ShapeDtypeStruct((rows + 8, 5 * LANES), F32),
            payload_shape,
            jax.ShapeDtypeStruct((feats, 4 * LANES + feats), BF16),
        ],
        in_specs=[hbm] * len(own),
        out_specs=[vmem] * 3,
        scratch_shapes=[
            pltpu.VMEM(own[0].shape, BF16),
            pltpu.VMEM(own[1].shape, F32),
            pltpu.VMEM((2, *own[2].shape), F32),
            pltpu.VMEM((4, *own[4].shape), BF16),
            pltpu.SemaphoreType.DMA((8,)),
        ],
        cost_estimate=pl.CostEstimate(flops=10**8, bytes_accessed=10**6, transcendentals=0),
        compiler_params=pltpu.CompilerParams(vmem_limit_bytes=START_LIMIT),
        name="start",
    )(*own)


def pair_kernel(keep, received, payload_ref, rates_ref):
    n_z, own_rows, width = received.shape
    rates_ref[...] = keep[n_z * own_rows :, 0:LANES]
    total = keep[0 : n_z * own_rows, :] + received[...].reshape(n_z * own_rows, width).astype(F32)
    extra = total[:, 4 * LANES :]
    squares = extra[:, 0:1] + extra[:, 1:2] + extra[:, 2:3]
    store([total[:, p * LANES : (p + 1) * LANES] for p in range(4)], squares, payload_ref)


def add_up(parts, halves):
    terms = [p[...].astype(F32) for p in parts]
    update = (terms[0] + terms[1]) + (terms[2] + terms[3])
    feats = halves[0].shape[1]
    return [
        (half.astype(F32) + update[:, n * feats : (n + 1) * feats]).astype(BF16)
        for n, half in enumerate(halves)
    ]


def middle_kernel(p0, p1, p2, p3, tok, gain, *refs):
    w, (bundle, payload_ref, x_ref) = refs[0:4], refs[4:]
    core = lax.axis_index("c")
    n_z, _, own_rows, feats = tok.shape
    rows = n_z * own_rows
    mine = tok[:, core].reshape(rows, feats)
    halves = add_up((p0, p1, p2, p3), [mine, bundle[0:rows, 4 * LANES :]])
    other_gain = sum(
        bundle[rows + 16 * n : rows + 16 * n + 16, 4 * LANES :][0:1].astype(F32) for n in range(3)
    )
    totals, squares = project(halves[0], gain[1:2, :], [v[1] for v in w])
    other_w = [bundle[:, p * LANES : (p + 1) * LANES] for p in range(4)]
    others, other_squares = project(halves[1], other_gain, other_w)
    store([t + o for t, o in zip(totals, others)], squares + other_squares, payload_ref)
    x_ref[0] = halves[0]
    x_ref[1] = halves[1]


def last_kernel(*refs):
    parts, (x_in, keep_ref, send_ref) = refs[0:4], refs[4:]
    halves = add_up(parts, [x_in[0], x_in[1]])
    keep_ref[...] = halves[0]
    send_ref[...] = halves[1]


def join_kernel(keep, received, out_ref):
    core = lax.axis_index("c")
    n_z, _, own_rows, feats = out_ref.shape
    out_ref[:, core] = keep[...].reshape(n_z, own_rows, feats)
    out_ref[:, 1 - core] = received[...].reshape(n_z, own_rows, feats)


def sigmoid(x):
    return 1.0 / (1.0 + jnp.exp(-x))


def mix_kernel(layer, arrived, rates, state, gated_ref, terms_ref):
    summed = arrived[0].astype(F32)
    for n in range(1, arrived.shape[0]):
        summed = summed + arrived[n].astype(F32)
    own_rows = summed.shape[0]
    extra = summed[:, 4 * LANES :]
    square = extra[:, 0:1] + extra[:, 1:2] + extra[:, 2:3]
    row_scale = lax.rsqrt(square / D + EPS)
    query_pre, forget_pre, value, gate_pre = [
        row_scale * summed[:, p * LANES : (p + 1) * LANES] for p in range(4)
    ]
    floor = rates[layer : layer + 1, :]
    query = query_pre * sigmoid(query_pre) * LANES ** (-0.5)
    forget = floor + (1.0 - floor) * sigmoid(forget_pre)
    key_in = (1.0 - floor) * sigmoid(-forget_pre)
    terms_ref[0] = forget
    terms_ref[1] = key_in
    terms_ref[2] = value
    columns = (query * forget).T
    fresh = jnp.sum(query * key_in, axis=1, keepdims=True) * value
    kept = [
        jnp.sum(state[layer, i, 0] * columns[:, i : i + 1], axis=0, keepdims=True)
        for i in range(own_rows)
    ]
    read = jnp.concatenate(kept, axis=0) + fresh
    read = read * lax.rsqrt(jnp.mean(read * read, axis=1, keepdims=True) + EPS)
    gate = gate_pre * sigmoid(gate_pre)
    gated = (read * rates[layer + 2 : layer + 3, :] * gate).astype(BF16)
    for n in range(gated_ref.shape[0]):
        gated_ref[n] = gated


def update_kernel(terms_a, terms_b, state, out_ref):
    def write(terms):
        forget = terms[0].T
        key_in = terms[1].T
        for i in range(state.shape[1]):
            value = terms[2, i : i + 1, :]
            out_ref[0, i, 0] = state[0, i, 0] * forget[:, i : i + 1] + key_in[:, i : i + 1] * value

    @pl.when(pl.program_id(0) == 0)
    def _():
        write(terms_a)

    @pl.when(pl.program_id(0) == 1)
    def _():
        write(terms_b)


def new_states(terms_a, terms_b, state):
    layers, seqs, heads, dk, dv = state.shape
    step = 8
    terms_spec = pl.BlockSpec((3, step, dk), lambda l, i: (0, i, 0))
    state_spec = pl.BlockSpec((1, step, heads, dk, dv), lambda l, i: (l, i, 0, 0, 0))
    return pl.pallas_call(
        update_kernel,
        out_shape=jax.ShapeDtypeStruct(state.shape, F32),
        grid=(layers, seqs // step),
        in_specs=[terms_spec, terms_spec, state_spec],
        out_specs=state_spec,
        cost_estimate=pl.CostEstimate(flops=10**7, bytes_accessed=2 * state.size * 4, transcendentals=0),
        compiler_params=pltpu.CompilerParams(vmem_limit_bytes=12 * 2**20),
        name="new_states",
    )(terms_a, terms_b, state)


def output_kernel(layer, heads, w_a, w_b, out_ref):
    my_x = lax.axis_index("x")
    n_x = heads.shape[0]
    rows = heads.shape[1] * heads.shape[2]
    for half, w in enumerate((w_a, w_b)):
        total = None
        for i in range(n_x):
            block = w[lax.rem(my_x - i + n_x, n_x), layer]
            product = jnp.dot(
                heads[i].reshape(rows, LANES), block, preferred_element_type=F32
            )
            total = product if total is None else total + product
        total = total.astype(BF16)
        feats = total.shape[1]
        out_ref[:, half * feats : (half + 1) * feats] = total


def spread(copies, axes):
    return lax.all_to_all(copies, axes, split_axis=0, concat_axis=0, tiled=True)


def per_device(
    tokens, norm_gain, w_query, w_forget, w_value, w_gate, floor_rate, head_gain, w_output, state
):
    n_z, n_x, n_y = lax.axis_size("z"), lax.axis_size("x"), lax.axis_size("y")
    batch, feats = tokens.shape
    own_rows = batch // (2 * n_z)
    rows = n_z * own_rows

    def swap(v):
        return lax.ppermute(v, "c", [(0, 1), (1, 0)])

    weights = (w_query, w_forget, w_value, w_gate)
    tok = tokens.reshape(n_z, 2, own_rows, feats)
    payload_shape = jax.ShapeDtypeStruct((n_z, own_rows, 5 * LANES), BF16)
    x_shape = jax.ShapeDtypeStruct((2, rows, feats), BF16)
    keep, send, bundle = start(
        payload_shape, rows, tok, norm_gain, floor_rate, head_gain, *weights
    )
    received = swap(send)
    payload, rates = call(
        pair_kernel, [payload_shape, jax.ShapeDtypeStruct((8, LANES), F32)],
        keep, received, flops=10**6,
    )
    bundle_b = swap(bundle)
    pieces = [w_output]
    for k in range(1, n_x):
        pieces.append(lax.ppermute(w_output, "x", [(i, (i + k) % n_x) for i in range(n_x)]))
    gathered = jnp.stack(pieces)
    w_out = (gathered, swap(gathered))

    terms = []
    for layer in range(2):
        arrived = spread(payload, "z")
        gated, term = call(
            functools.partial(mix_kernel, layer),
            [
                jax.ShapeDtypeStruct((n_x * n_z, own_rows, LANES), BF16),
                jax.ShapeDtypeStruct((3, own_rows, LANES), F32),
            ],
            arrived, rates, state, flops=10**7,
        )
        terms.append(term)
        heads = spread(gated, ("x", "z")).reshape(n_x, n_z, own_rows, LANES)
        (own,) = call(
            functools.partial(output_kernel, layer),
            [jax.ShapeDtypeStruct((rows, 2 * feats), BF16)],
            heads, *w_out, flops=10**8,
        )
        parts = [own]
        for k in range(1, n_y):
            parts.append(lax.ppermute(own, "y", [(i, i ^ k) for i in range(n_y)]))
        if layer == 0:
            payload, x = call(
                middle_kernel, [payload_shape, x_shape],
                *parts, tok, norm_gain, *weights, bundle_b, flops=10**8,
            )
    half = jax.ShapeDtypeStruct((rows, feats), BF16)
    keep, send = call(last_kernel, [half, half], *parts, x, flops=10**6)
    states = new_states(*terms, state)
    received = swap(send)
    (mixed,) = call(
        join_kernel, [jax.ShapeDtypeStruct((n_z, 2, own_rows, feats), BF16)],
        keep, received, flops=10**6,
    )
    return mixed.reshape(batch, feats), states


def solution(mesh):
    n_tp, n_dp = mesh.devices.shape
    fine = Mesh(mesh.devices.reshape(4, n_tp // 4, n_dp // 2, 2), ("y", "x", "z", "c"))
    dp, tp = ("z", "c"), ("y", "x")
    in_specs = (
        P(None, dp),
        P(None, dp),
        P(None, dp, tp),
        P(None, dp, tp),
        P(None, dp, tp),
        P(None, dp, tp),
        P(None, tp),
        P(),
        P(None, tp, dp),
        P(None, dp, tp, None, None),
    )
    out_specs = (P(None, dp), P(None, dp, tp, None, None))
    return jax.shard_map(
        per_device, mesh=fine, in_specs=in_specs, out_specs=out_specs, check_vma=False
    )
```

```python
import functools

import jax
import jax.numpy as jnp
from jax import lax
from jax.experimental import pallas as pl
from jax.experimental.pallas import tpu as pltpu
from jax.sharding import Mesh
from jax.sharding import PartitionSpec as P


D = 4096
EPS = 1e-06
BF16 = jnp.bfloat16
F32 = jnp.float32
LANES = 128


START_LIMIT = 56 * 2**20


def call(kernel, outs, *args, flops=0):
    vmem = pl.BlockSpec(memory_space=pltpu.VMEM)
    size = sum(a.size * a.dtype.itemsize for a in args)
    return pl.pallas_call(
        kernel,
        out_shape=outs,
        in_specs=[vmem] * len(args),
        out_specs=[vmem] * len(outs),
        cost_estimate=pl.CostEstimate(flops=flops, bytes_accessed=size, transcendentals=0),
        compiler_params=pltpu.CompilerParams(vmem_limit_bytes=12 * 2**20),
    )(*args)


def rounded(x):
    return x.astype(BF16).astype(F32)


def project(x, gain, weights):
    x = x.astype(F32)
    normed = (x * gain).astype(BF16)
    products = [jnp.dot(normed, w, preferred_element_type=F32) for w in weights]
    return products, jnp.sum(x * x, axis=1, keepdims=True)


def in_three(squares):
    high = rounded(squares)
    middle = rounded(squares - high)
    low = squares - high - middle
    lane = lax.broadcasted_iota(jnp.int32, (squares.shape[0], LANES), 1)
    return jnp.where(
        lane == 0, high, jnp.where(lane == 1, middle, jnp.where(lane == 2, low, 0.0))
    )


def store(totals, squares, payload_ref):
    n_z, own_rows, _ = payload_ref.shape
    for p, part in enumerate([*totals, in_three(squares)]):
        payload_ref[:, :, p * LANES : (p + 1) * LANES] = (
            part.astype(BF16).reshape(n_z, own_rows, LANES)
        )


def start_kernel(tok, gain, floor_rate, head_gain, *refs):
    w = refs[0:4]
    keep_ref, send_ref, bundle_ref, tok_here, gain_here, rates_here, w_here, sems = refs[4:]
    core = lax.axis_index("c")
    n_z, _, own_rows, feats = tok.shape
    rows = n_z * own_rows
    copies = [
        pltpu.make_async_copy(tok, tok_here, sems.at[0]),
        pltpu.make_async_copy(gain, gain_here, sems.at[1]),
        pltpu.make_async_copy(floor_rate, rates_here.at[0], sems.at[2]),
        pltpu.make_async_copy(head_gain, rates_here.at[1], sems.at[3]),
        *[pltpu.make_async_copy(w[p], w_here.at[p], sems.at[4 + p]) for p in range(4)],
    ]
    for copy in copies:
        copy.start()
    for copy in copies:
        copy.wait()
    weights = [w_here.at[p] for p in range(4)]
    gain_0 = gain_here[0:1, :]
    x = tok_here[:, 1 - core].reshape(rows, feats)
    bundle_ref[0:rows, 4 * LANES :] = x
    store(*project(x, gain_0, [v[0] for v in weights]), send_ref)
    x = tok_here[:, core].reshape(rows, feats)
    totals, squares = project(x, gain_0, [v[0] for v in weights])
    for p in range(4):
        keep_ref[0:rows, p * LANES : (p + 1) * LANES] = totals[p]
        bundle_ref[0:feats, p * LANES : (p + 1) * LANES] = weights[p][1]
    keep_ref[0:rows, 4 * LANES :] = in_three(squares)
    keep_ref[rows : rows + 2, 0:LANES] = rates_here[0]
    keep_ref[rows + 2 : rows + 4, 0:LANES] = rates_here[1]
    gain_1 = gain_here[1:2, :]
    high = rounded(gain_1)
    middle = rounded(gain_1 - high)
    for n, term in enumerate((high, middle, gain_1 - high - middle)):
        bundle_ref[rows + 16 * n : rows + 16 * n + 16, 4 * LANES :] = jnp.broadcast_to(
            term, (16, feats)
        ).astype(BF16)


def start(payload_shape, rows, *own):
    vmem = pl.BlockSpec(memory_space=pltpu.VMEM)
    hbm = pl.BlockSpec(memory_space=pltpu.HBM)
    feats = own[1].shape[1]
    return pl.pallas_call(
        start_kernel,
        out_shape=[
            jax.ShapeDtypeStruct((rows + 8, 5 * LANES), F32),
            payload_shape,
            jax.ShapeDtypeStruct((feats, 4 * LANES + feats), BF16),
        ],
        in_specs=[hbm] * len(own),
        out_specs=[vmem] * 3,
        scratch_shapes=[
            pltpu.VMEM(own[0].shape, BF16),
            pltpu.VMEM(own[1].shape, F32),
            pltpu.VMEM((2, *own[2].shape), F32),
            pltpu.VMEM((4, *own[4].shape), BF16),
            pltpu.SemaphoreType.DMA((8,)),
        ],
        cost_estimate=pl.CostEstimate(flops=10**9, bytes_accessed=10**6, transcendentals=0),
        compiler_params=pltpu.CompilerParams(vmem_limit_bytes=START_LIMIT),
        name="start",
    )(*own)


def lanes_kernel(out_ref):
    row = lax.broadcasted_iota(jnp.int32, out_ref.shape, 0)
    lane = lax.broadcasted_iota(jnp.int32, out_ref.shape, 1)
    out_ref[...] = jnp.where(row == lane, 1.0, 0.0)


def pair_kernel(keep, received, lanes, payload_ref, rates_ref):
    n_z, own_rows, width = received.shape
    rates_ref[...] = keep[n_z * own_rows :, 0:LANES]
    total = keep[0 : n_z * own_rows, :] + received[...].reshape(n_z * own_rows, width).astype(F32)
    extra = total[:, 4 * LANES :]
    squares = extra[:, 0:1] + extra[:, 1:2] + extra[:, 2:3]
    for p in range(4):
        payload_ref[:, :, p * LANES : (p + 1) * LANES] = (
            total[:, p * LANES : (p + 1) * LANES].astype(BF16).reshape(n_z, own_rows, LANES)
        )
    high = rounded(squares)
    middle = rounded(squares - high)
    terms = high * lanes[0:1] + middle * lanes[1:2] + (squares - high - middle) * lanes[2:3]
    payload_ref[:, :, 4 * LANES :] = terms.astype(BF16).reshape(n_z, own_rows, LANES)


def add_up(parts, halves):
    terms = [p[...].astype(F32) for p in parts]
    update = (terms[0] + terms[1]) + (terms[2] + terms[3])
    feats = halves[0].shape[1]
    return [
        (half.astype(F32) + update[:, n * feats : (n + 1) * feats]).astype(BF16)
        for n, half in enumerate(halves)
    ]


def middle_kernel(p0, p1, p2, p3, tok, gain, *refs):
    w, (bundle, payload_ref, x_ref) = refs[0:4], refs[4:]
    core = lax.axis_index("c")
    n_z, _, own_rows, feats = tok.shape
    rows = n_z * own_rows
    mine = tok[:, core].reshape(rows, feats)
    halves = add_up((p0, p1, p2, p3), [mine, bundle[0:rows, 4 * LANES :]])
    other_gain = sum(
        bundle[rows + 16 * n : rows + 16 * n + 16, 4 * LANES :][0:1].astype(F32) for n in range(3)
    )
    totals, squares = project(halves[0], gain[1:2, :], [v[1] for v in w])
    other_w = [bundle[:, p * LANES : (p + 1) * LANES] for p in range(4)]
    others, other_squares = project(halves[1], other_gain, other_w)
    store([t + o for t, o in zip(totals, others)], squares + other_squares, payload_ref)
    x_ref[0] = halves[0]
    x_ref[1] = halves[1]


def last_kernel(*refs):
    parts, (x_in, keep_ref, send_ref) = refs[0:4], refs[4:]
    halves = add_up(parts, [x_in[0], x_in[1]])
    keep_ref[...] = halves[0]
    send_ref[...] = halves[1]


def join_kernel(keep, received, out_ref):
    core = lax.axis_index("c")
    n_z, _, own_rows, feats = out_ref.shape
    out_ref[:, core] = keep[...].reshape(n_z, own_rows, feats)
    out_ref[:, 1 - core] = received[...].reshape(n_z, own_rows, feats)


def sigmoid(x):
    return 1.0 / (1.0 + jnp.exp(-x))


def mix_kernel(layer, arrived, rates, state, gated_ref, terms_ref):
    summed = arrived[0].astype(F32)
    for n in range(1, arrived.shape[0]):
        summed = summed + arrived[n].astype(F32)
    own_rows = summed.shape[0]
    extra = summed[:, 4 * LANES :]
    square = extra[:, 0:1] + extra[:, 1:2] + extra[:, 2:3]
    row_scale = lax.rsqrt(square / D + EPS)
    query_pre, forget_pre, value, gate_pre = [
        row_scale * summed[:, p * LANES : (p + 1) * LANES] for p in range(4)
    ]
    floor = rates[layer : layer + 1, :]
    query = query_pre * sigmoid(query_pre) * LANES ** (-0.5)
    forget = floor + (1.0 - floor) * sigmoid(forget_pre)
    key_in = (1.0 - floor) * sigmoid(-forget_pre)
    terms_ref[0] = forget
    terms_ref[1] = key_in
    terms_ref[2] = value
    columns = (query * forget).T
    fresh = jnp.sum(query * key_in, axis=1, keepdims=True) * value
    kept = [
        jnp.sum(state[layer, i, 0] * columns[:, i : i + 1], axis=0, keepdims=True)
        for i in range(own_rows)
    ]
    read = jnp.concatenate(kept, axis=0) + fresh
    read = read * lax.rsqrt(jnp.mean(read * read, axis=1, keepdims=True) + EPS)
    gate = gate_pre * sigmoid(gate_pre)
    gated = (read * rates[layer + 2 : layer + 3, :] * gate).astype(BF16)
    for n in range(gated_ref.shape[0]):
        gated_ref[n] = gated


def update_kernel(terms_a, terms_b, state, out_ref):
    def write(terms):
        forget = terms[0].T
        key_in = terms[1].T
        for i in range(state.shape[1]):
            value = terms[2, i : i + 1, :]
            out_ref[0, i, 0] = state[0, i, 0] * forget[:, i : i + 1] + key_in[:, i : i + 1] * value

    @pl.when(pl.program_id(0) == 0)
    def _():
        write(terms_a)

    @pl.when(pl.program_id(0) == 1)
    def _():
        write(terms_b)


def new_states(terms_a, terms_b, state):
    layers, seqs, heads, dk, dv = state.shape
    step = 8
    terms_spec = pl.BlockSpec((3, step, dk), lambda l, i: (0, i, 0))
    state_spec = pl.BlockSpec((1, step, heads, dk, dv), lambda l, i: (l, i, 0, 0, 0))
    return pl.pallas_call(
        update_kernel,
        out_shape=jax.ShapeDtypeStruct(state.shape, F32),
        grid=(layers, seqs // step),
        in_specs=[terms_spec, terms_spec, state_spec],
        out_specs=state_spec,
        cost_estimate=pl.CostEstimate(flops=10**7, bytes_accessed=2 * state.size * 4, transcendentals=0),
        compiler_params=pltpu.CompilerParams(vmem_limit_bytes=12 * 2**20),
        name="new_states",
    )(terms_a, terms_b, state)


def output_kernel(layer, heads, w_a, w_b, out_ref):
    my_x = lax.axis_index("x")
    n_x = heads.shape[0]
    rows = heads.shape[1] * heads.shape[2]
    for half, w in enumerate((w_a, w_b)):
        total = None
        for i in range(n_x):
            block = w[lax.rem(my_x - i + n_x, n_x), layer]
            product = jnp.dot(
                heads[i].reshape(rows, LANES), block, preferred_element_type=F32
            )
            total = product if total is None else total + product
        total = total.astype(BF16)
        feats = total.shape[1]
        out_ref[:, half * feats : (half + 1) * feats] = total


def spread(copies, axes):
    return lax.all_to_all(copies, axes, split_axis=0, concat_axis=0, tiled=True)


def per_device(
    tokens, norm_gain, w_query, w_forget, w_value, w_gate, floor_rate, head_gain, w_output, state
):
    n_z, n_x, n_y = lax.axis_size("z"), lax.axis_size("x"), lax.axis_size("y")
    batch, feats = tokens.shape
    own_rows = batch // (2 * n_z)
    rows = n_z * own_rows

    def swap(v):
        return lax.ppermute(v, "c", [(0, 1), (1, 0)])

    weights = (w_query, w_forget, w_value, w_gate)
    tok = tokens.reshape(n_z, 2, own_rows, feats)
    payload_shape = jax.ShapeDtypeStruct((n_z, own_rows, 5 * LANES), BF16)
    x_shape = jax.ShapeDtypeStruct((2, rows, feats), BF16)
    keep, send, bundle = start(
        payload_shape, rows, tok, norm_gain, floor_rate, head_gain, *weights
    )
    received = swap(send)
    (lanes,) = call(lanes_kernel, [jax.ShapeDtypeStruct((8, LANES), F32)], flops=10**9)
    payload, rates = call(
        pair_kernel, [payload_shape, jax.ShapeDtypeStruct((8, LANES), F32)],
        keep, received, lanes, flops=10**6,
    )
    bundle_b = swap(bundle)
    pieces = [w_output]
    for k in range(1, n_x):
        pieces.append(lax.ppermute(w_output, "x", [(i, (i + k) % n_x) for i in range(n_x)]))
    gathered = jnp.stack(pieces)
    w_out = (gathered, swap(gathered))

    terms = []
    for layer in range(2):
        arrived = spread(payload, "z")
        gated, term = call(
            functools.partial(mix_kernel, layer),
            [
                jax.ShapeDtypeStruct((n_x * n_z, own_rows, LANES), BF16),
                jax.ShapeDtypeStruct((3, own_rows, LANES), F32),
            ],
            arrived, rates, state, flops=10**7,
        )
        terms.append(term)
        heads = spread(gated, ("x", "z")).reshape(n_x, n_z, own_rows, LANES)
        (own,) = call(
            functools.partial(output_kernel, layer),
            [jax.ShapeDtypeStruct((rows, 2 * feats), BF16)],
            heads, *w_out, flops=10**8,
        )
        parts = [own]
        for k in range(1, n_y):
            parts.append(lax.ppermute(own, "y", [(i, i ^ k) for i in range(n_y)]))
        if layer == 0:
            payload, x = call(
                middle_kernel, [payload_shape, x_shape],
                *parts, tok, norm_gain, *weights, bundle_b, flops=10**8,
            )
    half = jax.ShapeDtypeStruct((rows, feats), BF16)
    keep, send = call(last_kernel, [half, half], *parts, x, flops=10**6)
    states = new_states(*terms, state)
    received = swap(send)
    (mixed,) = call(
        join_kernel, [jax.ShapeDtypeStruct((n_z, 2, own_rows, feats), BF16)],
        keep, received, flops=10**6,
    )
    return mixed.reshape(batch, feats), states


def solution(mesh):
    n_tp, n_dp = mesh.devices.shape
    fine = Mesh(mesh.devices.reshape(4, n_tp // 4, n_dp // 2, 2), ("y", "x", "z", "c"))
    dp, tp = ("z", "c"), ("y", "x")
    in_specs = (
        P(None, dp),
        P(None, dp),
        P(None, dp, tp),
        P(None, dp, tp),
        P(None, dp, tp),
        P(None, dp, tp),
        P(None, tp),
        P(),
        P(None, tp, dp),
        P(None, dp, tp, None, None),
    )
    out_specs = (P(None, dp), P(None, dp, tp, None, None))
    return jax.shard_map(
        per_device, mesh=fine, in_specs=in_specs, out_specs=out_specs, check_vma=False
    )
```

```python
import functools

import jax
import jax.numpy as jnp
from jax import lax
from jax.experimental import pallas as pl
from jax.experimental.pallas import tpu as pltpu
from jax.sharding import Mesh
from jax.sharding import PartitionSpec as P


D = 4096
EPS = 1e-06
BF16 = jnp.bfloat16
F32 = jnp.float32
LANES = 128


LANES_COST = 10**10


def call(kernel, outs, *args, flops=0):
    vmem = pl.BlockSpec(memory_space=pltpu.VMEM)
    size = sum(a.size * a.dtype.itemsize for a in args)
    return pl.pallas_call(
        kernel,
        out_shape=outs,
        in_specs=[vmem] * len(args),
        out_specs=[vmem] * len(outs),
        cost_estimate=pl.CostEstimate(flops=flops, bytes_accessed=size, transcendentals=0),
        compiler_params=pltpu.CompilerParams(vmem_limit_bytes=12 * 2**20),
    )(*args)


def rounded(x):
    return x.astype(BF16).astype(F32)


def project(x, gain, weights):
    x = x.astype(F32)
    normed = (x * gain).astype(BF16)
    products = [jnp.dot(normed, w, preferred_element_type=F32) for w in weights]
    return products, jnp.sum(x * x, axis=1, keepdims=True)


def in_three(squares, lanes):
    high = rounded(squares)
    middle = rounded(squares - high)
    low = squares - high - middle
    return high * lanes[0:1] + middle * lanes[1:2] + low * lanes[2:3]


def store(totals, squares, lanes, payload_ref):
    n_z, own_rows, _ = payload_ref.shape
    for p, part in enumerate([*totals, in_three(squares, lanes)]):
        payload_ref[:, :, p * LANES : (p + 1) * LANES] = (
            part.astype(BF16).reshape(n_z, own_rows, LANES)
        )


def start_kernel(lanes, tok, gain, floor_rate, head_gain, *refs):
    w, (keep_ref, send_ref, bundle_ref, rates_ref) = refs[0:4], refs[4:]
    core = lax.axis_index("c")
    n_z, _, own_rows, feats = tok.shape
    rows = n_z * own_rows
    weights = [v[0] for v in w]
    gain_0 = gain[0:1, :]
    x = tok[:, 1 - core].reshape(rows, feats)
    bundle_ref[0:rows, 4 * LANES :] = x
    store(*project(x, gain_0, weights), lanes, send_ref)
    x = tok[:, core].reshape(rows, feats)
    totals, squares = project(x, gain_0, weights)
    for p in range(4):
        keep_ref[:, p * LANES : (p + 1) * LANES] = totals[p]
        bundle_ref[:, p * LANES : (p + 1) * LANES] = w[p][1]
    keep_ref[:, 4 * LANES :] = in_three(squares, lanes)
    rates_ref[0:2] = floor_rate[...]
    rates_ref[2:4] = head_gain[...]
    gain_1 = gain[1:2, :]
    high = rounded(gain_1)
    middle = rounded(gain_1 - high)
    for n, term in enumerate((high, middle, gain_1 - high - middle)):
        bundle_ref[rows + 16 * n : rows + 16 * n + 16, 4 * LANES :] = jnp.broadcast_to(
            term, (16, feats)
        ).astype(BF16)


def lanes_kernel(out_ref):
    row = lax.broadcasted_iota(jnp.int32, out_ref.shape, 0)
    lane = lax.broadcasted_iota(jnp.int32, out_ref.shape, 1)
    out_ref[...] = jnp.where(row == lane, 1.0, 0.0)


def pair_kernel(lanes, keep, received, payload_ref):
    n_z, own_rows, width = received.shape
    total = keep[...] + received[...].reshape(n_z * own_rows, width).astype(F32)
    extra = total[:, 4 * LANES :]
    squares = extra[:, 0:1] + extra[:, 1:2] + extra[:, 2:3]
    parts = [total[:, p * LANES : (p + 1) * LANES] for p in range(4)]
    store(parts, squares, lanes, payload_ref)


def add_up(parts, halves):
    terms = [p[...].astype(F32) for p in parts]
    update = (terms[0] + terms[1]) + (terms[2] + terms[3])
    feats = halves[0].shape[1]
    return [
        (half.astype(F32) + update[:, n * feats : (n + 1) * feats]).astype(BF16)
        for n, half in enumerate(halves)
    ]


def middle_kernel(p0, p1, p2, p3, lanes, tok, gain, *refs):
    w, (bundle, payload_ref, x_ref) = refs[0:4], refs[4:]
    core = lax.axis_index("c")
    n_z, _, own_rows, feats = tok.shape
    rows = n_z * own_rows
    mine = tok[:, core].reshape(rows, feats)
    halves = add_up((p0, p1, p2, p3), [mine, bundle[0:rows, 4 * LANES :]])
    other_gain = sum(
        bundle[rows + 16 * n : rows + 16 * n + 16, 4 * LANES :][0:1].astype(F32) for n in range(3)
    )
    totals, squares = project(halves[0], gain[1:2, :], [v[1] for v in w])
    other_w = [bundle[:, p * LANES : (p + 1) * LANES] for p in range(4)]
    others, other_squares = project(halves[1], other_gain, other_w)
    store([t + o for t, o in zip(totals, others)], squares + other_squares, lanes, payload_ref)
    x_ref[0] = halves[0]
    x_ref[1] = halves[1]


def last_kernel(*refs):
    parts, (x_in, keep_ref, send_ref) = refs[0:4], refs[4:]
    halves = add_up(parts, [x_in[0], x_in[1]])
    keep_ref[...] = halves[0]
    send_ref[...] = halves[1]


def join_kernel(keep, received, out_ref):
    core = lax.axis_index("c")
    n_z, _, own_rows, feats = out_ref.shape
    out_ref[:, core] = keep[...].reshape(n_z, own_rows, feats)
    out_ref[:, 1 - core] = received[...].reshape(n_z, own_rows, feats)


def sigmoid(x):
    return 1.0 / (1.0 + jnp.exp(-x))


def mix_kernel(layer, arrived, rates, state, gated_ref, terms_ref):
    summed = arrived[0].astype(F32)
    for n in range(1, arrived.shape[0]):
        summed = summed + arrived[n].astype(F32)
    own_rows = summed.shape[0]
    extra = summed[:, 4 * LANES :]
    square = extra[:, 0:1] + extra[:, 1:2] + extra[:, 2:3]
    row_scale = lax.rsqrt(square / D + EPS)
    query_pre, forget_pre, value, gate_pre = [
        row_scale * summed[:, p * LANES : (p + 1) * LANES] for p in range(4)
    ]
    floor = rates[layer : layer + 1, :]
    query = query_pre * sigmoid(query_pre) * LANES ** (-0.5)
    forget = floor + (1.0 - floor) * sigmoid(forget_pre)
    key_in = (1.0 - floor) * sigmoid(-forget_pre)
    terms_ref[0] = forget
    terms_ref[1] = key_in
    terms_ref[2] = value
    columns = (query * forget).T
    fresh = jnp.sum(query * key_in, axis=1, keepdims=True) * value
    kept = [
        jnp.sum(state[layer, i, 0] * columns[:, i : i + 1], axis=0, keepdims=True)
        for i in range(own_rows)
    ]
    read = jnp.concatenate(kept, axis=0) + fresh
    read = read * lax.rsqrt(jnp.mean(read * read, axis=1, keepdims=True) + EPS)
    gate = gate_pre * sigmoid(gate_pre)
    gated = (read * rates[layer + 2 : layer + 3, :] * gate).astype(BF16)
    for n in range(gated_ref.shape[0]):
        gated_ref[n] = gated


def update_kernel(terms_a, terms_b, state, out_ref):
    def write(terms):
        forget = terms[0].T
        key_in = terms[1].T
        for i in range(state.shape[1]):
            value = terms[2, i : i + 1, :]
            out_ref[0, i, 0] = state[0, i, 0] * forget[:, i : i + 1] + key_in[:, i : i + 1] * value

    @pl.when(pl.program_id(0) == 0)
    def _():
        write(terms_a)

    @pl.when(pl.program_id(0) == 1)
    def _():
        write(terms_b)


def new_states(terms_a, terms_b, state):
    layers, seqs, heads, dk, dv = state.shape
    step = 8
    terms_spec = pl.BlockSpec((3, step, dk), lambda l, i: (0, i, 0))
    state_spec = pl.BlockSpec((1, step, heads, dk, dv), lambda l, i: (l, i, 0, 0, 0))
    return pl.pallas_call(
        update_kernel,
        out_shape=jax.ShapeDtypeStruct(state.shape, F32),
        grid=(layers, seqs // step),
        in_specs=[terms_spec, terms_spec, state_spec],
        out_specs=state_spec,
        cost_estimate=pl.CostEstimate(flops=10**7, bytes_accessed=2 * state.size * 4, transcendentals=0),
        compiler_params=pltpu.CompilerParams(vmem_limit_bytes=12 * 2**20),
        name="new_states",
    )(terms_a, terms_b, state)


def output_kernel(layer, heads, w_a, w_b, out_ref):
    my_x = lax.axis_index("x")
    n_x = heads.shape[0]
    rows = heads.shape[1] * heads.shape[2]
    for half, w in enumerate((w_a, w_b)):
        total = None
        for i in range(n_x):
            block = w[lax.rem(my_x - i + n_x, n_x), layer]
            product = jnp.dot(
                heads[i].reshape(rows, LANES), block, preferred_element_type=F32
            )
            total = product if total is None else total + product
        total = total.astype(BF16)
        feats = total.shape[1]
        out_ref[:, half * feats : (half + 1) * feats] = total


def spread(copies, axes):
    return lax.all_to_all(copies, axes, split_axis=0, concat_axis=0, tiled=True)


def per_device(
    tokens, norm_gain, w_query, w_forget, w_value, w_gate, floor_rate, head_gain, w_output, state
):
    n_z, n_x, n_y = lax.axis_size("z"), lax.axis_size("x"), lax.axis_size("y")
    batch, feats = tokens.shape
    own_rows = batch // (2 * n_z)
    rows = n_z * own_rows

    def swap(v):
        return lax.ppermute(v, "c", [(0, 1), (1, 0)])

    weights = (w_query, w_forget, w_value, w_gate)
    tok = tokens.reshape(n_z, 2, own_rows, feats)
    payload_shape = jax.ShapeDtypeStruct((n_z, own_rows, 5 * LANES), BF16)
    x_shape = jax.ShapeDtypeStruct((2, rows, feats), BF16)
    (lanes,) = call(lanes_kernel, [jax.ShapeDtypeStruct((8, LANES), F32)], flops=LANES_COST)
    keep, send, bundle, rates = call(
        start_kernel,
        [
            jax.ShapeDtypeStruct((rows, 5 * LANES), F32),
            payload_shape,
            jax.ShapeDtypeStruct((feats, 4 * LANES + feats), BF16),
            jax.ShapeDtypeStruct((8, LANES), F32),
        ],
        lanes, tok, norm_gain, floor_rate, head_gain, *weights, flops=10**8,
    )
    received = swap(send)
    (payload,) = call(pair_kernel, [payload_shape], lanes, keep, received, flops=10**6)
    bundle_b = swap(bundle)
    pieces = [w_output]
    for k in range(1, n_x):
        pieces.append(lax.ppermute(w_output, "x", [(i, (i + k) % n_x) for i in range(n_x)]))
    gathered = jnp.stack(pieces)
    w_out = (gathered, swap(gathered))

    terms = []
    for layer in range(2):
        arrived = spread(payload, "z")
        gated, term = call(
            functools.partial(mix_kernel, layer),
            [
                jax.ShapeDtypeStruct((n_x * n_z, own_rows, LANES), BF16),
                jax.ShapeDtypeStruct((3, own_rows, LANES), F32),
            ],
            arrived, rates, state, flops=10**7,
        )
        terms.append(term)
        heads = spread(gated, ("x", "z")).reshape(n_x, n_z, own_rows, LANES)
        (own,) = call(
            functools.partial(output_kernel, layer),
            [jax.ShapeDtypeStruct((rows, 2 * feats), BF16)],
            heads, *w_out, flops=10**8,
        )
        parts = [own]
        for k in range(1, n_y):
            parts.append(lax.ppermute(own, "y", [(i, i ^ k) for i in range(n_y)]))
        if layer == 0:
            payload, x = call(
                middle_kernel, [payload_shape, x_shape],
                *parts, lanes, tok, norm_gain, *weights, bundle_b, flops=10**8,
            )
    half = jax.ShapeDtypeStruct((rows, feats), BF16)
    keep, send = call(last_kernel, [half, half], *parts, x, flops=10**6)
    states = new_states(*terms, state)
    received = swap(send)
    (mixed,) = call(
        join_kernel, [jax.ShapeDtypeStruct((n_z, 2, own_rows, feats), BF16)],
        keep, received, flops=10**6,
    )
    return mixed.reshape(batch, feats), states


def solution(mesh):
    n_tp, n_dp = mesh.devices.shape
    fine = Mesh(mesh.devices.reshape(4, n_tp // 4, n_dp // 2, 2), ("y", "x", "z", "c"))
    dp, tp = ("z", "c"), ("y", "x")
    in_specs = (
        P(None, dp),
        P(None, dp),
        P(None, dp, tp),
        P(None, dp, tp),
        P(None, dp, tp),
        P(None, dp, tp),
        P(None, tp),
        P(),
        P(None, tp, dp),
        P(None, dp, tp, None, None),
    )
    out_specs = (P(None, dp), P(None, dp, tp, None, None))
    return jax.shard_map(
        per_device, mesh=fine, in_specs=in_specs, out_specs=out_specs, check_vma=False
    )
```

```python
import functools

import jax
import jax.numpy as jnp
from jax import lax
from jax.experimental import pallas as pl
from jax.experimental.pallas import tpu as pltpu
from jax.sharding import Mesh
from jax.sharding import PartitionSpec as P


D = 4096
EPS = 1e-06
BF16 = jnp.bfloat16
F32 = jnp.float32
LANES = 128


LANES_COST = 10**10


def call(kernel, outs, *args, flops=0):
    vmem = pl.BlockSpec(memory_space=pltpu.VMEM)
    size = sum(a.size * a.dtype.itemsize for a in args)
    return pl.pallas_call(
        kernel,
        out_shape=outs,
        in_specs=[vmem] * len(args),
        out_specs=[vmem] * len(outs),
        cost_estimate=pl.CostEstimate(flops=flops, bytes_accessed=size, transcendentals=0),
        compiler_params=pltpu.CompilerParams(vmem_limit_bytes=12 * 2**20),
    )(*args)


def rounded(x):
    return x.astype(BF16).astype(F32)


def project(x, gain, weights):
    x = x.astype(F32)
    normed = (x * gain).astype(BF16)
    products = [jnp.dot(normed, w, preferred_element_type=F32) for w in weights]
    return products, jnp.sum(x * x, axis=1, keepdims=True)


def in_three(squares, lanes):
    high = rounded(squares)
    middle = rounded(squares - high)
    low = squares - high - middle
    return high * lanes[0:1] + middle * lanes[1:2] + low * lanes[2:3]


def store(totals, squares, lanes, payload_ref):
    n_z, own_rows, _ = payload_ref.shape
    for p, part in enumerate([*totals, in_three(squares, lanes)]):
        payload_ref[:, :, p * LANES : (p + 1) * LANES] = (
            part.astype(BF16).reshape(n_z, own_rows, LANES)
        )


def start_kernel(lanes, tok, gain, floor_rate, head_gain, *refs):
    w, (keep_ref, send_ref, bundle_ref, rates_ref) = refs[0:4], refs[4:]
    core = lax.axis_index("c")
    n_z, _, own_rows, feats = tok.shape
    rows = n_z * own_rows
    weights = [v[0] for v in w]
    gain_0 = gain[0:1, :]
    x = tok[:, 1 - core].reshape(rows, feats)
    bundle_ref[0:rows, 4 * LANES :] = x
    store(*project(x, gain_0, weights), lanes, send_ref)
    x = tok[:, core].reshape(rows, feats)
    totals, squares = project(x, gain_0, weights)
    for p in range(4):
        keep_ref[:, p * LANES : (p + 1) * LANES] = totals[p]
        bundle_ref[:, p * LANES : (p + 1) * LANES] = w[p][1]
    keep_ref[:, 4 * LANES :] = in_three(squares, lanes)
    rates_ref[0:2] = floor_rate[...]
    rates_ref[2:4] = head_gain[...]
    gain_1 = gain[1:2, :]
    high = rounded(gain_1)
    middle = rounded(gain_1 - high)
    for n, term in enumerate((high, middle, gain_1 - high - middle)):
        bundle_ref[rows + 16 * n : rows + 16 * n + 16, 4 * LANES :] = jnp.broadcast_to(
            term, (16, feats)
        ).astype(BF16)


def lanes_kernel(out_ref):
    row = lax.broadcasted_iota(jnp.int32, out_ref.shape, 0)
    lane = lax.broadcasted_iota(jnp.int32, out_ref.shape, 1)
    out_ref[...] = jnp.where(row == lane, 1.0, 0.0)


def pair_kernel(lanes, keep, received, payload_ref):
    n_z, own_rows, width = received.shape
    total = keep[...] + received[...].reshape(n_z * own_rows, width).astype(F32)
    extra = total[:, 4 * LANES :]
    squares = extra[:, 0:1] + extra[:, 1:2] + extra[:, 2:3]
    parts = [total[:, p * LANES : (p + 1) * LANES] for p in range(4)]
    store(parts, squares, lanes, payload_ref)


def add_up(parts, halves):
    terms = [p[...].astype(F32) for p in parts]
    update = (terms[0] + terms[1]) + (terms[2] + terms[3])
    feats = halves[0].shape[1]
    return [
        (half.astype(F32) + update[:, n * feats : (n + 1) * feats]).astype(BF16)
        for n, half in enumerate(halves)
    ]


def middle_kernel(p0, p1, p2, p3, lanes, tok, gain, *refs):
    w, (bundle, payload_ref, x_ref) = refs[0:4], refs[4:]
    core = lax.axis_index("c")
    n_z, _, own_rows, feats = tok.shape
    rows = n_z * own_rows
    mine = tok[:, core].reshape(rows, feats)
    halves = add_up((p0, p1, p2, p3), [mine, bundle[0:rows, 4 * LANES :]])
    other_gain = sum(
        bundle[rows + 16 * n : rows + 16 * n + 16, 4 * LANES :][0:1].astype(F32) for n in range(3)
    )
    totals, squares = project(halves[0], gain[1:2, :], [v[1] for v in w])
    other_w = [bundle[:, p * LANES : (p + 1) * LANES] for p in range(4)]
    others, other_squares = project(halves[1], other_gain, other_w)
    store([t + o for t, o in zip(totals, others)], squares + other_squares, lanes, payload_ref)
    x_ref[0] = halves[0]
    x_ref[1] = halves[1]


def last_kernel(*refs):
    parts, (x_in, keep_ref, send_ref) = refs[0:4], refs[4:]
    halves = add_up(parts, [x_in[0], x_in[1]])
    keep_ref[...] = halves[0]
    send_ref[...] = halves[1]


def join_kernel(keep, received, out_ref):
    core = lax.axis_index("c")
    n_z, _, own_rows, feats = out_ref.shape
    out_ref[:, core] = keep[...].reshape(n_z, own_rows, feats)
    out_ref[:, 1 - core] = received[...].reshape(n_z, own_rows, feats)


def sigmoid(x):
    return 1.0 / (1.0 + jnp.exp(-x))


def mix_kernel(layer, arrived, rates, state, gated_ref, terms_ref):
    summed = arrived[0].astype(F32)
    for n in range(1, arrived.shape[0]):
        summed = summed + arrived[n].astype(F32)
    own_rows = summed.shape[0]
    extra = summed[:, 4 * LANES :]
    square = extra[:, 0:1] + extra[:, 1:2] + extra[:, 2:3]
    row_scale = lax.rsqrt(square / D + EPS)
    query_pre, forget_pre, value, gate_pre = [
        row_scale * summed[:, p * LANES : (p + 1) * LANES] for p in range(4)
    ]
    floor = rates[layer : layer + 1, :]
    query = query_pre * sigmoid(query_pre) * LANES ** (-0.5)
    forget = floor + (1.0 - floor) * sigmoid(forget_pre)
    key_in = (1.0 - floor) * sigmoid(-forget_pre)
    terms_ref[0] = forget
    terms_ref[1] = key_in
    terms_ref[2] = value
    columns = (query * forget).T
    fresh = jnp.sum(query * key_in, axis=1, keepdims=True) * value
    kept = [
        jnp.sum(state[layer, i, 0] * columns[:, i : i + 1], axis=0, keepdims=True)
        for i in range(own_rows)
    ]
    read = jnp.concatenate(kept, axis=0) + fresh
    read = read * lax.rsqrt(jnp.mean(read * read, axis=1, keepdims=True) + EPS)
    gate = gate_pre * sigmoid(gate_pre)
    gated = (read * rates[layer + 2 : layer + 3, :] * gate).astype(BF16)
    for n in range(gated_ref.shape[0]):
        gated_ref[n] = gated


def update_kernel(terms_a, terms_b, state, out_ref):
    def write(terms):
        forget = terms[0].T
        key_in = terms[1].T
        for i in range(state.shape[1]):
            value = terms[2, i : i + 1, :]
            out_ref[0, i, 0] = state[0, i, 0] * forget[:, i : i + 1] + key_in[:, i : i + 1] * value

    @pl.when(pl.program_id(0) == 0)
    def _():
        write(terms_a)

    @pl.when(pl.program_id(0) == 1)
    def _():
        write(terms_b)


def new_states(terms_a, terms_b, state):
    layers, seqs, heads, dk, dv = state.shape
    step = 8
    terms_spec = pl.BlockSpec((3, step, dk), lambda l, i: (0, i, 0))
    state_spec = pl.BlockSpec((1, step, heads, dk, dv), lambda l, i: (l, i, 0, 0, 0))
    return pl.pallas_call(
        update_kernel,
        out_shape=jax.ShapeDtypeStruct(state.shape, F32),
        grid=(layers, seqs // step),
        in_specs=[terms_spec, terms_spec, state_spec],
        out_specs=state_spec,
        cost_estimate=pl.CostEstimate(flops=10**7, bytes_accessed=2 * state.size * 4, transcendentals=0),
        compiler_params=pltpu.CompilerParams(vmem_limit_bytes=12 * 2**20),
        name="new_states",
    )(terms_a, terms_b, state)


def output_kernel(layer, heads, *refs):
    pieces, out_ref = refs[:-1], refs[-1]
    my_x = lax.axis_index("x")
    n_x = heads.shape[0]
    rows = heads.shape[1] * heads.shape[2]
    feats = pieces[0].shape[3]
    for half in range(2):
        total = None
        for k in range(n_x):
            head = heads[lax.rem(my_x - k + n_x, n_x)].reshape(rows, LANES)
            product = jnp.dot(head, pieces[k][half, layer], preferred_element_type=F32)
            total = product if total is None else total + product
        out_ref[:, half * feats : (half + 1) * feats] = total.astype(BF16)


def spread(copies, axes):
    return lax.all_to_all(copies, axes, split_axis=0, concat_axis=0, tiled=True)


def per_device(
    tokens, norm_gain, w_query, w_forget, w_value, w_gate, floor_rate, head_gain, w_output, state
):
    n_z, n_x, n_y = lax.axis_size("z"), lax.axis_size("x"), lax.axis_size("y")
    batch, feats = tokens.shape
    own_rows = batch // (2 * n_z)
    rows = n_z * own_rows

    def swap(v):
        return lax.ppermute(v, "c", [(0, 1), (1, 0)])

    weights = (w_query, w_forget, w_value, w_gate)
    tok = tokens.reshape(n_z, 2, own_rows, feats)
    payload_shape = jax.ShapeDtypeStruct((n_z, own_rows, 5 * LANES), BF16)
    x_shape = jax.ShapeDtypeStruct((2, rows, feats), BF16)
    (lanes,) = call(lanes_kernel, [jax.ShapeDtypeStruct((8, LANES), F32)], flops=LANES_COST)
    keep, send, bundle, rates = call(
        start_kernel,
        [
            jax.ShapeDtypeStruct((rows, 5 * LANES), F32),
            payload_shape,
            jax.ShapeDtypeStruct((feats, 4 * LANES + feats), BF16),
            jax.ShapeDtypeStruct((8, LANES), F32),
        ],
        lanes, tok, norm_gain, floor_rate, head_gain, *weights, flops=10**8,
    )
    received = swap(send)
    (payload,) = call(pair_kernel, [payload_shape], lanes, keep, received, flops=10**6)
    bundle_b = swap(bundle)
    w_other = swap(w_output)
    both = jnp.stack([w_output, w_other])
    w_out = [both]
    for k in range(1, n_x):
        w_out.append(lax.ppermute(both, "x", [(i, (i + k) % n_x) for i in range(n_x)]))

    terms = []
    for layer in range(2):
        arrived = spread(payload, "z")
        gated, term = call(
            functools.partial(mix_kernel, layer),
            [
                jax.ShapeDtypeStruct((n_x * n_z, own_rows, LANES), BF16),
                jax.ShapeDtypeStruct((3, own_rows, LANES), F32),
            ],
            arrived, rates, state, flops=10**7,
        )
        terms.append(term)
        heads = spread(gated, ("x", "z")).reshape(n_x, n_z, own_rows, LANES)
        (own,) = call(
            functools.partial(output_kernel, layer),
            [jax.ShapeDtypeStruct((rows, 2 * feats), BF16)],
            heads, *w_out, flops=10**8,
        )
        parts = [own]
        for k in range(1, n_y):
            parts.append(lax.ppermute(own, "y", [(i, i ^ k) for i in range(n_y)]))
        if layer == 0:
            payload, x = call(
                middle_kernel, [payload_shape, x_shape],
                *parts, lanes, tok, norm_gain, *weights, bundle_b, flops=10**8,
            )
    half = jax.ShapeDtypeStruct((rows, feats), BF16)
    keep, send = call(last_kernel, [half, half], *parts, x, flops=10**6)
    states = new_states(*terms, state)
    received = swap(send)
    (mixed,) = call(
        join_kernel, [jax.ShapeDtypeStruct((n_z, 2, own_rows, feats), BF16)],
        keep, received, flops=10**6,
    )
    return mixed.reshape(batch, feats), states


def solution(mesh):
    n_tp, n_dp = mesh.devices.shape
    fine = Mesh(mesh.devices.reshape(4, n_tp // 4, n_dp // 2, 2), ("y", "x", "z", "c"))
    dp, tp = ("z", "c"), ("y", "x")
    in_specs = (
        P(None, dp),
        P(None, dp),
        P(None, dp, tp),
        P(None, dp, tp),
        P(None, dp, tp),
        P(None, dp, tp),
        P(None, tp),
        P(),
        P(None, tp, dp),
        P(None, dp, tp, None, None),
    )
    out_specs = (P(None, dp), P(None, dp, tp, None, None))
    return jax.shard_map(
        per_device, mesh=fine, in_specs=in_specs, out_specs=out_specs, check_vma=False
    )
```

```python
import functools

import jax
import jax.numpy as jnp
from jax import lax
from jax.experimental import pallas as pl
from jax.experimental.pallas import tpu as pltpu
from jax.sharding import Mesh
from jax.sharding import PartitionSpec as P


D = 4096
EPS = 1e-06
BF16 = jnp.bfloat16
F32 = jnp.float32
LANES = 128


LANES_COST = 10**10


def call(kernel, outs, *args, flops=0):
    vmem = pl.BlockSpec(memory_space=pltpu.VMEM)
    size = sum(a.size * a.dtype.itemsize for a in args)
    return pl.pallas_call(
        kernel,
        out_shape=outs,
        in_specs=[vmem] * len(args),
        out_specs=[vmem] * len(outs),
        cost_estimate=pl.CostEstimate(flops=flops, bytes_accessed=size, transcendentals=0),
        compiler_params=pltpu.CompilerParams(vmem_limit_bytes=12 * 2**20),
    )(*args)


def rounded(x):
    return x.astype(BF16).astype(F32)


def project(x, gain, weights):
    x = x.astype(F32)
    normed = (x * gain).astype(BF16)
    products = [jnp.dot(normed, w, preferred_element_type=F32) for w in weights]
    return products, jnp.sum(x * x, axis=1, keepdims=True)


def in_three(squares, lanes):
    high = rounded(squares)
    middle = rounded(squares - high)
    low = squares - high - middle
    return high * lanes[0:1] + middle * lanes[1:2] + low * lanes[2:3]


def store(totals, squares, lanes, payload_ref):
    n_z, own_rows, _ = payload_ref.shape
    for p, part in enumerate([*totals, in_three(squares, lanes)]):
        payload_ref[:, :, p * LANES : (p + 1) * LANES] = (
            part.astype(BF16).reshape(n_z, own_rows, LANES)
        )


def start_kernel(lanes, tok, gain, floor_rate, head_gain, *refs):
    w, (keep_ref, send_ref, bundle_ref, rates_ref) = refs[0:4], refs[4:]
    core = lax.axis_index("c")
    n_z, _, own_rows, feats = tok.shape
    rows = n_z * own_rows
    weights = [v[0] for v in w]
    gain_0 = gain[0:1, :]
    x = tok[:, 1 - core].reshape(rows, feats)
    bundle_ref[0:rows, 4 * LANES :] = x
    store(*project(x, gain_0, weights), lanes, send_ref)
    x = tok[:, core].reshape(rows, feats)
    totals, squares = project(x, gain_0, weights)
    for p in range(4):
        keep_ref[:, p * LANES : (p + 1) * LANES] = totals[p]
        bundle_ref[:, p * LANES : (p + 1) * LANES] = w[p][1]
    keep_ref[:, 4 * LANES :] = in_three(squares, lanes)
    rates_ref[0:2] = floor_rate[...]
    rates_ref[2:4] = head_gain[...]
    gain_1 = gain[1:2, :]
    high = rounded(gain_1)
    middle = rounded(gain_1 - high)
    for n, term in enumerate((high, middle, gain_1 - high - middle)):
        bundle_ref[rows + 16 * n : rows + 16 * n + 16, 4 * LANES :] = jnp.broadcast_to(
            term, (16, feats)
        ).astype(BF16)


def lanes_kernel(out_ref):
    row = lax.broadcasted_iota(jnp.int32, out_ref.shape, 0)
    lane = lax.broadcasted_iota(jnp.int32, out_ref.shape, 1)
    out_ref[...] = jnp.where(row == lane, 1.0, 0.0)


def pair_kernel(lanes, keep, received, payload_ref):
    n_z, own_rows, width = received.shape
    total = keep[...] + received[...].reshape(n_z * own_rows, width).astype(F32)
    extra = total[:, 4 * LANES :]
    squares = extra[:, 0:1] + extra[:, 1:2] + extra[:, 2:3]
    parts = [total[:, p * LANES : (p + 1) * LANES] for p in range(4)]
    store(parts, squares, lanes, payload_ref)


def add_up(parts, halves):
    terms = [p[...].astype(F32) for p in parts]
    update = (terms[0] + terms[1]) + (terms[2] + terms[3])
    feats = halves[0].shape[1]
    return [
        (half.astype(F32) + update[:, n * feats : (n + 1) * feats]).astype(BF16)
        for n, half in enumerate(halves)
    ]


def middle_kernel(p0, p1, p2, p3, lanes, tok, gain, *refs):
    w, (bundle, payload_ref, x_ref) = refs[0:4], refs[4:]
    core = lax.axis_index("c")
    n_z, _, own_rows, feats = tok.shape
    rows = n_z * own_rows
    mine = tok[:, core].reshape(rows, feats)
    halves = add_up((p0, p1, p2, p3), [mine, bundle[0:rows, 4 * LANES :]])
    other_gain = sum(
        bundle[rows + 16 * n : rows + 16 * n + 16, 4 * LANES :][0:1].astype(F32) for n in range(3)
    )
    totals, squares = project(halves[0], gain[1:2, :], [v[1] for v in w])
    other_w = [bundle[:, p * LANES : (p + 1) * LANES] for p in range(4)]
    others, other_squares = project(halves[1], other_gain, other_w)
    store([t + o for t, o in zip(totals, others)], squares + other_squares, lanes, payload_ref)
    x_ref[0] = halves[0]
    x_ref[1] = halves[1]


def last_kernel(*refs):
    parts, (x_in, keep_ref, send_ref) = refs[0:4], refs[4:]
    halves = add_up(parts, [x_in[0], x_in[1]])
    keep_ref[...] = halves[0]
    send_ref[...] = halves[1]


def join_kernel(keep, received, out_ref):
    core = lax.axis_index("c")
    n_z, _, own_rows, feats = out_ref.shape
    out_ref[:, core] = keep[...].reshape(n_z, own_rows, feats)
    out_ref[:, 1 - core] = received[...].reshape(n_z, own_rows, feats)


def sigmoid(x):
    return 1.0 / (1.0 + jnp.exp(-x))


def mix_kernel(layer, arrived, rates, state, gated_ref, terms_ref):
    summed = arrived[0].astype(F32)
    for n in range(1, arrived.shape[0]):
        summed = summed + arrived[n].astype(F32)
    own_rows = summed.shape[0]
    extra = summed[:, 4 * LANES :]
    square = extra[:, 0:1] + extra[:, 1:2] + extra[:, 2:3]
    row_scale = lax.rsqrt(square / D + EPS)
    query_pre, forget_pre, value, gate_pre = [
        row_scale * summed[:, p * LANES : (p + 1) * LANES] for p in range(4)
    ]
    floor = rates[layer : layer + 1, :]
    query = query_pre * sigmoid(query_pre) * LANES ** (-0.5)
    forget = floor + (1.0 - floor) * sigmoid(forget_pre)
    key_in = (1.0 - floor) * sigmoid(-forget_pre)
    terms_ref[0] = forget
    terms_ref[1] = key_in
    terms_ref[2] = value
    columns = (query * forget).T
    fresh = jnp.sum(query * key_in, axis=1, keepdims=True) * value
    kept = [
        jnp.sum(state[layer, i, 0] * columns[:, i : i + 1], axis=0, keepdims=True)
        for i in range(own_rows)
    ]
    read = jnp.concatenate(kept, axis=0) + fresh
    read = read * lax.rsqrt(jnp.mean(read * read, axis=1, keepdims=True) + EPS)
    gate = gate_pre * sigmoid(gate_pre)
    gated = (read * rates[layer + 2 : layer + 3, :] * gate).astype(BF16)
    for n in range(gated_ref.shape[0]):
        gated_ref[n] = gated


def update_kernel(terms_a, terms_b, state, out_ref):
    def write(terms):
        forget = terms[0].T
        key_in = terms[1].T
        for i in range(state.shape[1]):
            value = terms[2, i : i + 1, :]
            out_ref[0, i, 0] = state[0, i, 0] * forget[:, i : i + 1] + key_in[:, i : i + 1] * value

    @pl.when(pl.program_id(0) == 0)
    def _():
        write(terms_a)

    @pl.when(pl.program_id(0) == 1)
    def _():
        write(terms_b)


def new_states(terms_a, terms_b, state):
    layers, seqs, heads, dk, dv = state.shape
    step = 8
    terms_spec = pl.BlockSpec((3, step, dk), lambda l, i: (0, i, 0))
    state_spec = pl.BlockSpec((1, step, heads, dk, dv), lambda l, i: (l, i, 0, 0, 0))
    return pl.pallas_call(
        update_kernel,
        out_shape=jax.ShapeDtypeStruct(state.shape, F32),
        grid=(layers, seqs // step),
        in_specs=[terms_spec, terms_spec, state_spec],
        out_specs=state_spec,
        cost_estimate=pl.CostEstimate(flops=10**7, bytes_accessed=2 * state.size * 4, transcendentals=0),
        compiler_params=pltpu.CompilerParams(vmem_limit_bytes=12 * 2**20),
        name="new_states",
    )(terms_a, terms_b, state)


def output_kernel(layer, heads, *refs):
    pieces, out_ref = refs[:-1], refs[-1]
    my_x = lax.axis_index("x")
    n_x = heads.shape[0]
    rows = heads.shape[1] * heads.shape[2]
    feats = pieces[0].shape[3]
    for half in range(2):
        products = [
            jnp.dot(
                heads[lax.rem(my_x - k + n_x, n_x)].reshape(rows, LANES),
                pieces[k][half, layer],
                preferred_element_type=F32,
            )
            for k in range(n_x)
        ]
        total = (products[0] + products[2]) + (products[1] + products[3])
        out_ref[:, half * feats : (half + 1) * feats] = total.astype(BF16)


def spread(copies, axes):
    return lax.all_to_all(copies, axes, split_axis=0, concat_axis=0, tiled=True)


def per_device(
    tokens, norm_gain, w_query, w_forget, w_value, w_gate, floor_rate, head_gain, w_output, state
):
    n_z, n_x, n_y = lax.axis_size("z"), lax.axis_size("x"), lax.axis_size("y")
    batch, feats = tokens.shape
    own_rows = batch // (2 * n_z)
    rows = n_z * own_rows

    def swap(v):
        return lax.ppermute(v, "c", [(0, 1), (1, 0)])

    weights = (w_query, w_forget, w_value, w_gate)
    tok = tokens.reshape(n_z, 2, own_rows, feats)
    payload_shape = jax.ShapeDtypeStruct((n_z, own_rows, 5 * LANES), BF16)
    x_shape = jax.ShapeDtypeStruct((2, rows, feats), BF16)
    (lanes,) = call(lanes_kernel, [jax.ShapeDtypeStruct((8, LANES), F32)], flops=LANES_COST)
    keep, send, bundle, rates = call(
        start_kernel,
        [
            jax.ShapeDtypeStruct((rows, 5 * LANES), F32),
            payload_shape,
            jax.ShapeDtypeStruct((feats, 4 * LANES + feats), BF16),
            jax.ShapeDtypeStruct((8, LANES), F32),
        ],
        lanes, tok, norm_gain, floor_rate, head_gain, *weights, flops=10**8,
    )
    received = swap(send)
    (payload,) = call(pair_kernel, [payload_shape], lanes, keep, received, flops=10**6)
    bundle_b = swap(bundle)
    w_other = swap(w_output)
    both = jnp.stack([w_output, w_other])
    w_out = [both]
    for k in range(1, n_x):
        w_out.append(lax.ppermute(both, "x", [(i, (i + k) % n_x) for i in range(n_x)]))

    terms = []
    for layer in range(2):
        arrived = spread(payload, "z")
        gated, term = call(
            functools.partial(mix_kernel, layer),
            [
                jax.ShapeDtypeStruct((n_x * n_z, own_rows, LANES), BF16),
                jax.ShapeDtypeStruct((3, own_rows, LANES), F32),
            ],
            arrived, rates, state, flops=10**7,
        )
        terms.append(term)
        heads = spread(gated, ("x", "z")).reshape(n_x, n_z, own_rows, LANES)
        (own,) = call(
            functools.partial(output_kernel, layer),
            [jax.ShapeDtypeStruct((rows, 2 * feats), BF16)],
            heads, *w_out, flops=10**8,
        )
        parts = [own]
        for k in range(1, n_y):
            parts.append(lax.ppermute(own, "y", [(i, i ^ k) for i in range(n_y)]))
        if layer == 0:
            payload, x = call(
                middle_kernel, [payload_shape, x_shape],
                *parts, lanes, tok, norm_gain, *weights, bundle_b, flops=10**8,
            )
    half = jax.ShapeDtypeStruct((rows, feats), BF16)
    keep, send = call(last_kernel, [half, half], *parts, x, flops=10**6)
    states = new_states(*terms, state)
    received = swap(send)
    (mixed,) = call(
        join_kernel, [jax.ShapeDtypeStruct((n_z, 2, own_rows, feats), BF16)],
        keep, received, flops=10**6,
    )
    return mixed.reshape(batch, feats), states


def solution(mesh):
    n_tp, n_dp = mesh.devices.shape
    fine = Mesh(mesh.devices.reshape(4, n_tp // 4, n_dp // 2, 2), ("y", "x", "z", "c"))
    dp, tp = ("z", "c"), ("y", "x")
    in_specs = (
        P(None, dp),
        P(None, dp),
        P(None, dp, tp),
        P(None, dp, tp),
        P(None, dp, tp),
        P(None, dp, tp),
        P(None, tp),
        P(),
        P(None, tp, dp),
        P(None, dp, tp, None, None),
    )
    out_specs = (P(None, dp), P(None, dp, tp, None, None))
    return jax.shard_map(
        per_device, mesh=fine, in_specs=in_specs, out_specs=out_specs, check_vma=False
    )
```
